512 devices in a mesh: ep: 32 (over z, core), tp: 16 (over y, x).
Axes of the slice: x: 4, y: 4, z: 16, core: 2. Of those that a mesh axis runs over, the one named last changes fastest.
Arguments:
- mix_input: bfloat16 [4096, 2048], P('ep'), may hold values from -8 to 8
- expert_input: bfloat16 [4096, 2048], P('ep'), may hold values from -8 to 8
- mix_gain: float32 [2048], replicated, may hold values from 0.1 to 1.9
- moe_gain: float32 [2048], replicated, may hold values from 0.1 to 1.9
- pool_in: bfloat16 [2048, 1024], P(None, 'tp'), may hold values from -0.125 to 0.125
- pool_scale: float32 [1024], P('tp'), may hold values from 0.25 to 10
- pool_gain: float32 [1024], P('tp'), may hold values from 0.1 to 1.9
- pool_out: bfloat16 [1024, 2048], P(None, 'tp'), may hold values from -0.1875 to 0.1875
- route: int32 [4096, 4], P('ep'), may hold values from 0 to 31, all different within a row; in each aligned block of 128 rows (0 to 127, 128 to 255, ...) at most 32 rows name the same one
- route_score: float32 [4096, 4], P('ep'), may hold values from 0.05 to 1
- expert_gate: bfloat16 [32, 2048, 2048], P('ep', None, 'tp'), may hold values from -0.125 to 0.125
- expert_up: bfloat16 [32, 2048, 2048], P('ep', None, 'tp'), may hold values from -0.125 to 0.125
- expert_down: bfloat16 [32, 2048, 2048], P('ep', 'tp'), may hold values from -0.1875 to 0.1875
- shared_gate: bfloat16 [2048, 2048], P(None, 'tp'), may hold values from -0.125 to 0.125
- shared_up: bfloat16 [2048, 2048], P(None, 'tp'), may hold values from -0.125 to 0.125
- shared_down: bfloat16 [2048, 2048], P(None, 'tp'), may hold values from -0.125 to 0.125
Outputs:
- mix_out: bfloat16 [4096, 2048], P('ep', 'tp')
- moe_out: bfloat16 [4096, 2048], P('ep', 'tp')
The draws below stay inside these ranges and needn't reach their ends.
Inputs may be any that keep to these rules, and one draw needn't show every extreme that they name: `route`: each row names 4 different experts. In the rows of one index of ep (aligned blocks of 128 rows) no expert is named more than 32 times, a bound that some block reaches.
All inputs are finite; a program needn't handle non-finite values.
Results may differ from the reference program's by a relative error of at most 0.014.
Values may be sent and summed in bfloat16 or wider, within the bound.
A program may use at most 64 MiB of HBM per device.

```python
import math
import jax
import jax.numpy as jnp
import numpy as np
from jax import lax

D = 2048
POOL = 1024
FE = 2048
FS = 2048
TOP_K = 4
TOK_B = 128
EXPERTS = 32
CAP = 32
TOKENS_A = 4096
TOKENS_B = 4096
N_EP = 32
N_TP = 16


def spread_rows(key, rows, cols):
    keys = jax.random.split(key, 3)
    row_scale = jnp.exp(jax.random.uniform(keys[0], (rows, 1), jnp.float32, math.log(0.3), math.log(3.0)))
    col_scale = jnp.exp(jax.random.uniform(keys[1], (1, cols), jnp.float32, math.log(0.3), math.log(3.0)))
    base = jax.random.normal(keys[2], (rows, cols), jnp.float32)
    return jnp.clip(base * row_scale * col_scale, -8.0, 8.0).astype(jnp.bfloat16)


def draw_mix_input(key, part):
    return spread_rows(jax.random.fold_in(key, 11), TOKENS_A, D)


def draw_expert_input(key, part):
    return spread_rows(jax.random.fold_in(key, 23), TOKENS_B, D)


def draw_pool_scale(key, part):
    channel = jnp.arange(POOL, dtype=jnp.float32) / POOL
    factor = jnp.exp(jax.random.uniform(jax.random.fold_in(key, 37), (POOL,), jnp.float32, math.log(0.5), math.log(2.0)))
    rising = jnp.exp(math.log(6.0) * channel)
    return 0.5 * rising * factor


def with_spikes(values, own_key, source, target, blocks, factor):
    def block_of(axis_at):
        return (jnp.arange(values.shape[axis_at]) // (values.shape[axis_at] // blocks)).reshape((-1,) + (1,) * (values.ndim - 1 - axis_at))

    near = jax.random.permutation(own_key, blocks)[block_of(target)]
    other_side = (block_of(target) + blocks // 2) % blocks
    return jnp.where((block_of(source) == near) | (block_of(source) == other_side), factor * values, values)


def steps_of(own_key, extent, cuts, low, top_value):
    loudness, own = 1.0, jax.random.fold_in(own_key, 6)
    for axis_at, blocks in cuts:
        steps = jnp.exp(jax.random.uniform(jax.random.fold_in(own, axis_at), (blocks,), jnp.float32, low / len(cuts), top_value / len(cuts)))
        loudness = loudness * jnp.repeat(steps, extent[axis_at] // blocks).reshape([-1 if axis == axis_at else 1 for axis in range(len(extent))])
    return loudness


def routed_block(own_key, own, number, rows, number_of, top, reach, slope):
    order = jax.random.permutation(own_key, number_of)
    heavy_load, usual = load_shares(number_of, rows * top, reach, slope, True), load_shares(number_of, rows * top, reach, slope, False)
    places = jnp.arange(number_of)

    def named(tallies, turn):
        used = int((tallies > 0).sum())
        fixed = max(1, used // 4)
        passed = fixed + (places - fixed + turn * (used - fixed)) % max(1, number_of - fixed)
        return jnp.zeros((number_of,), jnp.int32).at[order[jnp.where(places < fixed, places, passed)]].set(jnp.asarray(tallies, jnp.int32))

    tallies = jnp.where(number % 4 == 0, named(heavy_load, number // 4), named(usual, number - number // 4 - 1))
    mixed = jax.random.permutation(jax.random.fold_in(own, 3), number_of)
    source_of, receiver = mixed[0:number_of // 2 * 2:2], mixed[1:number_of // 2 * 2:2]
    slack = jnp.minimum(tallies[source_of] - 1, reach - tallies[receiver]) // 2
    slack = jnp.where((source_of == order[0]) | (receiver == order[0]) | (tallies[receiver] == 0), 0, jnp.maximum(slack, 0))
    passed = jax.random.randint(jax.random.fold_in(own, 4), (number_of // 2,), 0, 1 << 20) % (slack + 1)
    tallies = tallies.at[source_of].add(-passed).at[receiver].add(passed)
    items = jnp.searchsorted(jnp.cumsum(tallies), jnp.arange(rows * top), side="right").astype(jnp.int32)
    grid = items.reshape(top, rows).T
    grid = grid[jax.random.permutation(jax.random.fold_in(own, 1), rows)]
    turn = jax.random.randint(jax.random.fold_in(own, 2), (rows, 1), 0, top)
    return jnp.take_along_axis(grid, (jnp.arange(top)[None, :] + turn) % top, axis=1)


def load_shares(number_of, total, most, skew, full):
    loads = [(1 << 20) // math.isqrt(grade ** skew) + 1 for grade in range(1, number_of + 1)]
    largest = most if full else min(most, max(-(-total // number_of), total * loads[0] // sum(loads)))
    least = 1 if total - largest >= number_of - 1 else 0
    given, rest = [largest] + [least] * (number_of - 1), total - largest - least * (number_of - 1)
    while rest > 0:
        candidates = [i for i in range(1, number_of) if given[i] < largest] or [i for i in range(1, number_of) if given[i] < most]
        mass, budget = sum([loads[i] for i in candidates]), rest
        for i in candidates:
            more = min(most - given[i], max(1, budget * loads[i] // mass), rest)
            given[i] = given[i] + more
            rest = rest - more
    return np.array(given)


def bell_draw(stream_key, shape, spread, bound, pieces=(), kind=jnp.bfloat16):
    values = spread * jax.random.normal(stream_key, shape, jnp.float32)
    if pieces:
        values = values * steps_of(stream_key, shape, pieces, -0.22, 0.18)
    return jnp.clip(values, -bound, bound).astype(kind)


def gaussian_with(own_key, dims, deviation, reach, pieces, heavy, held_as=jnp.bfloat16):
    values = deviation * jax.random.normal(own_key, dims, jnp.float32)
    if pieces:
        values = values * steps_of(own_key, dims, pieces, -0.22, 0.18)
    return jnp.clip(with_spikes(values, jax.random.fold_in(own_key, 3), *heavy), -reach, reach).astype(held_as)


def setup_inputs(seed: int = 0) -> dict:
    arg_keys = jax.random.split(jax.random.key(seed), 17)
    mix_input = draw_mix_input(jax.random.fold_in(arg_keys[16], 71), 0)
    expert_input = draw_expert_input(jax.random.fold_in(arg_keys[16], 71), 0)
    mix_gain = jnp.clip(1.0 + 0.18 * jax.random.normal(arg_keys[2], (D,), jnp.float32), 0.1, 1.9)
    moe_gain = jnp.clip(1.0 + 0.18 * jax.random.normal(arg_keys[3], (D,), jnp.float32), 0.1, 1.9)
    pool_in = bell_draw(arg_keys[4], (D, POOL), D ** -0.5, 0.125, ((1, 16),))
    pool_scale = draw_pool_scale(jax.random.fold_in(arg_keys[16], 71), 0)
    pool_gain = jnp.clip(1.0 + 0.18 * jax.random.normal(arg_keys[6], (POOL,), jnp.float32), 0.1, 1.9)
    pool_out = bell_draw(arg_keys[7], (POOL, D), POOL ** -0.5, 0.1875, ((1, 16),))
    route_keys = jax.random.split(jax.random.fold_in(arg_keys[8], 1), TOKENS_B // TOK_B)
    route_turns = jax.random.permutation(jax.random.fold_in(arg_keys[8], 3), TOKENS_B // TOK_B)
    route = jax.vmap(lambda own, number: routed_block(jax.random.fold_in(arg_keys[8], 2), own, number, TOK_B, EXPERTS, TOP_K, CAP, 2))(route_keys, route_turns).reshape((TOKENS_B, TOP_K))
    route_score = jnp.clip(0.05 + 0.95 * jax.random.uniform(arg_keys[9], (TOKENS_B, TOP_K), jnp.float32) ** steps_of(arg_keys[9], (TOKENS_B, TOP_K), ((0, 32),), -0.2, 0.2), 0.05, 1.0)
    expert_gate = bell_draw(arg_keys[10], (EXPERTS, D, FE), D ** -0.5, 0.125, ((0, 32), (2, 16)))
    expert_up = bell_draw(arg_keys[11], (EXPERTS, D, FE), D ** -0.5, 0.125, ((0, 32), (2, 16)))
    expert_down = gaussian_with(arg_keys[12], (EXPERTS, FE, D), FE ** -0.5, 0.1875, ((0, 32), (1, 16)), (1, 2, 16, 2.0))
    shared_gate = bell_draw(arg_keys[13], (D, FS), D ** -0.5, 0.125, ((1, 16),))
    shared_up = bell_draw(arg_keys[14], (D, FS), D ** -0.5, 0.125, ((1, 16),))
    shared_down = bell_draw(arg_keys[15], (FS, D), FS ** -0.5, 0.125, ((1, 16),))
    return {"mix_input": mix_input, "expert_input": expert_input, "mix_gain": mix_gain, "moe_gain": moe_gain, "pool_in": pool_in, "pool_scale": pool_scale, "pool_gain": pool_gain, "pool_out": pool_out, "route": route, "route_score": route_score, "expert_gate": expert_gate, "expert_up": expert_up, "expert_down": expert_down, "shared_gate": shared_gate, "shared_up": shared_up, "shared_down": shared_down}


epsilon = 1e-06
reach_rows = 15
window_widths = (2, 4, 8, 16)

def row_norm(rows, gain):
    values = rows.astype(jnp.float32)
    scale = lax.rsqrt(lax.optimization_barrier(jnp.mean(values * values, axis=-1, keepdims=True)) + epsilon)
    return (values * scale * gain.astype(jnp.float32)).astype(jnp.bfloat16)

def window_means(extended, position, group, n_rows):
    total = jnp.zeros((n_rows, extended.shape[1]), jnp.float32)
    result = jnp.zeros((n_rows, extended.shape[1]), jnp.float32)
    for lag in range(16):
        total = total + extended[reach_rows - lag:reach_rows - lag + n_rows]
        for index, width in enumerate(window_widths):
            if lag + 1 == width:
                count = jnp.minimum(position, float(width))[:, None]
                result = jnp.where(group[None, :] == index, total / count, result)
    return result - extended[reach_rows:]

def reference(mix_input, expert_input, mix_gain, moe_gain, pool_in, pool_scale, pool_gain, pool_out, route, route_score, expert_gate, expert_up, expert_down, shared_gate, shared_up, shared_down):
    mix_norm = row_norm(mix_input, mix_gain)
    pool_input = jnp.dot(mix_norm, pool_in, preferred_element_type=jnp.float32).astype(jnp.bfloat16)
    extended = jnp.concatenate([jnp.zeros((reach_rows, POOL), jnp.float32), pool_input.astype(jnp.float32)], axis=0)
    position = jnp.arange(1, TOKENS_A + 1, dtype=jnp.int32).astype(jnp.float32)
    group = jnp.arange(POOL, dtype=jnp.int32) // (POOL // 4)
    scaled = window_means(extended, position, group, TOKENS_A) * pool_scale
    pooled_norm = (scaled * lax.rsqrt(lax.optimization_barrier(jnp.mean(scaled * scaled, axis=1, keepdims=True)) + epsilon) * pool_gain).astype(jnp.bfloat16)
    mix_out = jnp.dot(pooled_norm, pool_out, preferred_element_type=jnp.float32).astype(jnp.bfloat16)
    moe_norm = row_norm(expert_input, moe_gain)
    weights = 2.5 * route_score / lax.optimization_barrier(jnp.sum(route_score, axis=1, keepdims=True))
    most_rows = CAP * N_EP

    def one_expert(routed, expert):
        hit = route == expert
        taken = jnp.any(hit, axis=1)
        order = jnp.argsort(jnp.where(taken, 0, 1).astype(jnp.int32), stable=True)[:most_rows].astype(jnp.int32)
        live = taken[order]
        rows = moe_norm[order]
        gate = jnp.dot(rows, expert_gate[expert], preferred_element_type=jnp.float32)
        upper = jnp.dot(rows, expert_up[expert], preferred_element_type=jnp.float32)
        hidden = (jax.nn.silu(gate) * upper).astype(jnp.bfloat16)
        blocks = hidden.reshape(most_rows, N_TP, FE // N_TP).astype(jnp.float32)
        down = expert_down[expert].reshape(N_TP, FE // N_TP, D).astype(jnp.float32)
        partial_value = jnp.einsum('rpf,pfd->rpd', blocks, down).astype(jnp.bfloat16)
        result = lax.optimization_barrier(jnp.sum(partial_value.astype(jnp.float32), axis=1)).astype(jnp.bfloat16)
        factor = lax.optimization_barrier(jnp.sum(jnp.where(hit, weights, 0.0), axis=1))[order] * live
        routed = routed.at[order].add(result.astype(jnp.float32) * factor[:, None])
        return (routed, None)
    routed, _ = lax.scan(one_expert, jnp.zeros((TOKENS_B, D), jnp.float32), jnp.arange(EXPERTS, dtype=jnp.int32))
    shared_hidden = (jax.nn.silu(jnp.dot(moe_norm, shared_gate, preferred_element_type=jnp.float32)) * jnp.dot(moe_norm, shared_up, preferred_element_type=jnp.float32)).astype(jnp.bfloat16)
    shared = jnp.dot(shared_hidden, shared_down, preferred_element_type=jnp.float32)
    moe_out = (routed + shared).astype(jnp.bfloat16)
    return (mix_out, moe_out)
```

```python
import functools

import jax
import jax.numpy as jnp
from jax import lax
from jax.experimental import pallas as pl
from jax.experimental.pallas import tpu as pltpu
from jax.sharding import PartitionSpec as P

MESH = pl.DeviceIdType.MESH
F32, BF16 = jnp.float32, jnp.bfloat16
EPS = 1e-06
SIDE = 4
LANES = 128


def dot(a, b):
    return jnp.dot(a, b, preferred_element_type=F32)


def silu_mul(gate, upper):
    return gate / (1.0 + jnp.exp(-gate)) * upper


class Sems:
    def __init__(self, send, recv):
        self.send, self.recv, self.used = send, recv, 0

    def take(self):
        at = self.used
        self.used += 1
        return self.send.at[at], self.recv.at[at]


def kernel(
    n_pairs,
    xe_ref, xm_hbm, mix_gain_ref, moe_gain_ref, pin_hbm, pscale_ref, pgain_ref, pout_hbm, route_ref, score_ref,
    eg_hbm, eu_hbm, ed_hbm, sg_hbm, su_hbm, sd_hbm,
    mix_out_ref, moe_out_ref,
    xm, wgu, wd, sgu, sd, pin, po2, mn, mm, sel, chi, clo, outgoing, x_all, part, q_a, q_b, y_own, back,
    opp1, main1, opp2, main2, halo_out, halo_in, sq_out, sq_in,
    load_sems, send_sems, recv_sems, z_send, z_recv, zb_send, zb_recv, sq_send, sq_recv,
):
    n_ep, n_tp = lax.axis_size("ep"), lax.axis_size("tp")
    ep, tp = lax.axis_index("ep"), lax.axis_index("tp")
    n_z = n_ep // 2
    z, core = ep // 2, ep % 2
    my, mx = tp // SIDE, tp % SIDE
    tok, width = xe_ref.shape
    rows_all = outgoing.shape[0]
    cap = rows_all // n_ep
    sems = Sems(send_sems, recv_sems)

    def slot_place(i):
        pair, other = i // 2, i % 2
        far = (pair + 1) // 2
        step = jnp.where(pair % 2 == 1, far, n_z - far)
        return step, other

    def peer_to(i):
        step, other = slot_place(i)
        return ((z + step) % n_z) * 2 + (core + other) % 2

    def peer_from(i):
        step, other = slot_place(i)
        return ((z + n_z - step) % n_z) * 2 + (core + other) % 2

    barrier = pltpu.get_barrier_semaphore()

    @pl.loop(1, n_ep)
    def _(i):
        pl.semaphore_signal(barrier, inc=1, device_id={"ep": (ep + i) % n_ep, "tp": tp}, device_id_type=MESH)

    @pl.loop(1, n_tp)
    def _(i):
        pl.semaphore_signal(barrier, inc=1, device_id={"ep": ep, "tp": (tp + i) % n_tp}, device_id_type=MESH)

    loads = {}
    for at, (name, src, dst) in enumerate((
        ("xm", xm_hbm, xm),
        ("pin", pin_hbm, pin),
        ("sg", sg_hbm, sgu.at[:, 0:LANES]),
        ("su", su_hbm, sgu.at[:, LANES:2 * LANES]),
        ("eg", eg_hbm.at[0], wgu.at[:, 0:LANES]),
        ("eu", eu_hbm.at[0], wgu.at[:, LANES:2 * LANES]),
        ("ed", ed_hbm.at[0], wd),
        ("po_a", pout_hbm, po2.at[:, 0]),
        ("po_b", pout_hbm, po2.at[:, 1]),
        ("sd", sd_hbm, sd),
    )):
        loads[name] = pltpu.make_async_copy(src, dst, load_sems.at[at])
        loads[name].start()

    def row_norm(src, gain_ref, dst):
        @pl.loop(0, tok // 16)
        def _(b):
            at = pl.ds(pl.multiple_of(b * 16, 16), 16)
            values = src[at, :].astype(F32)
            scale = lax.rsqrt(jnp.mean(values * values, axis=-1, keepdims=True) + EPS)
            dst[at, :] = (values * scale * gain_ref[...]).astype(BF16)

    row_norm(xe_ref, moe_gain_ref, mn)

    top = route_ref.shape[1]
    lane = lax.broadcasted_iota(jnp.int32, (tok, LANES), 1)
    table = jnp.zeros((tok, LANES), F32)
    for k in range(top):
        table = jnp.where(lane == k, route_ref[:, k:k + 1].astype(F32), table)
        table = jnp.where(lane == top + k, score_ref[:, k:k + 1], table)
    table = table.T
    slot_i = lax.broadcasted_iota(jnp.int32, (n_ep, tok), 0)
    pair_i, other_i = slot_i // 2, slot_i % 2
    far_i = (pair_i + 1) // 2
    step_i = jnp.where(pair_i % 2 == 1, far_i, n_z - far_i)
    expert_i = (((z + step_i) % n_z) * 2 + (core + other_i) % 2).astype(F32)
    total = table[top:top + 1, :]
    for k in range(1, top):
        total = total + table[top + k:top + k + 1, :]
    hit = jnp.zeros((n_ep, tok), F32)
    weight = jnp.zeros((n_ep, tok), F32)
    for k in range(top):
        same = expert_i == table[k:k + 1, :]
        hit = jnp.where(same, 1.0, hit)
        weight = jnp.where(same, 2.5 * table[top + k:top + k + 1, :] / total, weight)
    before = (
        lax.broadcasted_iota(jnp.int32, (tok, tok), 0) < lax.broadcasted_iota(jnp.int32, (tok, tok), 1)
    )
    rank = dot(hit.astype(BF16), jnp.where(before, 1.0, 0.0).astype(BF16))
    place = jnp.where(hit > 0.0, rank, -1.0)
    slot_row = lax.broadcasted_iota(jnp.int32, (cap, tok), 0).astype(F32)
    for i in range(n_ep):
        sel[i * cap:(i + 1) * cap, :] = jnp.where(place[i:i + 1, :] == slot_row, 1.0, 0.0).astype(BF16)

    share = mn[:, pl.ds(pl.multiple_of(tp * LANES, LANES), LANES)]
    outgoing[...] = dot(sel[...], share).astype(BF16)
    x_all[my, mx, 0:cap, :] = outgoing[0:cap, :]

    pl.semaphore_wait(barrier, n_ep - 1 + n_tp - 1)

    per_chunk = n_ep // (2 * n_pairs)

    @pl.loop(1, n_ep)
    def _(i):
        at = pl.ds(pl.multiple_of(i * cap, cap), cap)
        pltpu.make_async_remote_copy(
            src_ref=outgoing.at[at], dst_ref=x_all.at[my, mx, at], send_sem=z_send, recv_sem=z_recv.at[i // per_chunk],
            device_id={"ep": peer_to(i), "tp": tp}, device_id_type=MESH,
        ).start()

    loads["xm"].wait()
    row_norm(xm, mix_gain_ref, mm)
    loads["pin"].wait()
    narrow = pin.shape[1]
    pooled_in = dot(mm[...], pin[...])
    pooled_in = jnp.concatenate([pooled_in, jnp.zeros((tok, LANES - narrow), F32)], axis=1).astype(BF16)
    halo_out[...] = pooled_in[tok - 16:, :]
    halo_sem = sems.take()
    halo = pltpu.make_async_remote_copy(
        src_ref=halo_out, dst_ref=halo_in, send_sem=halo_sem[0], recv_sem=halo_sem[1],
        device_id={"ep": (ep + 1) % n_ep, "tp": tp}, device_id_type=MESH,
    )
    halo.start()

    loads["sg"].wait()
    loads["su"].wait()
    both = dot(mn[...], sgu[...])
    shared_rows = slice(rows_all, rows_all + tok)
    x_all[my, mx, shared_rows, :] = silu_mul(both[:, :LANES], both[:, LANES:]).astype(BF16)

    def copy(src, dst, where):
        send, recv = sems.take()
        made = pltpu.make_async_remote_copy(
            src_ref=src, dst_ref=dst, send_sem=send, recv_sem=recv, device_id=where, device_id_type=MESH
        )
        sent.append(made)
        return made

    sent = [halo]
    x_ring = lambda step: {"ep": ep, "tp": my * SIDE + (mx + step) % SIDE}
    y_ring = lambda step: {"ep": ep, "tp": ((my + step) % SIDE) * SIDE + mx}

    class Ring:
        def __init__(self, view, me, ring, start, count):
            self.view, self.me, self.ring, self.start_row, self.count = view, me, ring, start, count

        def unit(self, step, part=None):
            half = self.count // 2
            lo, n = {None: (0, self.count), 0: (0, half), 1: (half, half)}[part]
            return self.view((self.me + step) % SIDE, pl.ds(self.start_row + lo, n))

        def start(self):
            own = self.unit(0)
            self.right = copy(own, own, self.ring(1))
            self.left = copy(own, own, self.ring(SIDE - 1))
            self.right.start()
            self.left.start()

        def relay(self):
            first, second = self.unit(SIDE - 1, 0), self.unit(1, 1)
            self.right.wait_recv()
            self.on_right = copy(first, first, self.ring(1))
            self.on_right.start()
            self.left.wait_recv()
            self.on_left = copy(second, second, self.ring(SIDE - 1))
            self.on_left.start()

        def finish(self):
            self.on_right.wait_recv()
            self.on_left.wait_recv()

    class Gather:
        def __init__(self, start, count, x_first):
            along_x = lambda i, at: x_all.at[my, i, at]
            along_y = lambda i, at: x_all.at[i, mx, at]
            whole_y = lambda i, at: x_all.at[i, :, at]
            whole_x = lambda i, at: x_all.at[:, i, at]
            if x_first:
                self.one = Ring(along_x, mx, x_ring, start, count)
                self.two = Ring(whole_y, my, y_ring, start, count)
            else:
                self.one = Ring(along_y, my, y_ring, start, count)
                self.two = Ring(whole_x, mx, x_ring, start, count)

    def gather_pair(a, b):
        return Gather(*a, True), Gather(*b, False)

    shared_gather = Gather(rows_all, tok, True)
    shared_gather.one.start()

    halo.wait_recv()
    carried = jnp.where(ep > 0, halo_in[...].astype(F32), 0.0)
    ext = jnp.concatenate([carried, pooled_in.astype(F32)], axis=0)
    sums, chosen, window = ext, None, 1
    for index in range(4):
        sums = sums + pltpu.roll(sums, window, 0)
        window *= 2
        chosen = sums if chosen is None else jnp.where(my >= index, sums, chosen)
    position = (ep * tok + lax.broadcasted_iota(jnp.int32, (tok, LANES), 0) + 1).astype(F32)
    widest = lax.shift_left(2, my).astype(F32)
    zeros_right = jnp.zeros((1, LANES - narrow), F32)
    pscale = jnp.concatenate([pscale_ref[...], zeros_right], axis=1)
    pgain = jnp.concatenate([pgain_ref[...], zeros_right], axis=1)
    scaled = (chosen[16:, :] / jnp.minimum(position, widest) - pooled_in.astype(F32)) * pscale
    squares = jnp.sum(scaled * scaled, axis=1, keepdims=True)
    squares = jnp.broadcast_to(squares, (tok, LANES)).T[0:8, :]
    sq_out[...] = squares

    @pl.loop(1, n_tp)
    def _(i):
        pltpu.make_async_remote_copy(
            src_ref=sq_out, dst_ref=sq_in.at[i - 1], send_sem=sq_send, recv_sem=sq_recv,
            device_id={"ep": ep, "tp": (tp + i) % n_tp}, device_id_type=MESH,
        ).start()

    high = weight.astype(BF16).astype(F32)
    low = weight - high
    for i in range(n_ep):
        at = slice(i * cap, (i + 1) * cap)
        same = place[i:i + 1, :] == slot_row
        chi[at, :] = jnp.where(same, high[i:i + 1, :], 0.0).astype(BF16)
        clo[at, :] = jnp.where(same, low[i:i + 1, :], 0.0).astype(BF16)

    shared_gather.one.relay()
    pltpu.make_async_copy(sq_in, sq_in, sq_recv).wait()
    for i in range(n_tp - 1):
        squares = squares + sq_in[i]
    squares = jnp.broadcast_to(squares[0:1, :], (tok, LANES)).T
    pooled = (scaled * lax.rsqrt(squares / (narrow * n_tp) + EPS) * pgain).astype(BF16).astype(F32)
    packed = pooled[:tok // 2, :] + pltpu.roll(pooled[tok // 2:, :], narrow, 1)
    pool_start = rows_all + tok
    x_all[my, mx, pool_start:pool_start + tok // 2, :] = packed.astype(BF16)
    pool_gather = Gather(pool_start, tok // 2, False)
    pool_gather.one.start()
    shared_gather.one.finish()
    shared_gather.two.start()
    pool_gather.one.relay()
    pool_gather.one.finish()
    pool_gather.two.start()

    loads["eg"].wait()
    loads["eu"].wait()
    loads["ed"].wait()

    count = rows_all // (2 * n_pairs)
    half = count // 2

    class RingSum:
        def __init__(self, view, me, ring, opp, main, start):
            self.view, self.me, self.ring, self.opp, self.main, self.start_row = view, me, ring, opp, main, start

        def unit(self, step, part):
            lo, n = {None: (0, count), 0: (0, half), 1: (half, half)}[part]
            return self.view((self.me + step) % SIDE, pl.ds(self.start_row + lo, n))

        def into(self, side, part):
            at = pl.ds(part * half, half)
            return self.main.at[(side,) + (slice(None),) * (len(self.main.shape) - 3) + (at,)]

        def start(self):
            self.opp_right = copy(self.unit(2, 0), self.opp.at[0], self.ring(1))
            self.opp_left = copy(self.unit(2, 1), self.opp.at[1], self.ring(SIDE - 1))
            self.far_right = copy(self.unit(1, 1), self.into(0, 1), self.ring(1))
            self.far_left = copy(self.unit(SIDE - 1, 0), self.into(1, 0), self.ring(SIDE - 1))
            for made in (self.opp_right, self.opp_left, self.far_right, self.far_left):
                made.start()

        def add(self, unit, extra):
            unit[...] = (unit[...].astype(F32) + extra[...].astype(F32)).astype(BF16)

        def relay(self):
            self.opp_right.wait_recv()
            self.add(self.unit(1, 0), self.opp.at[0])
            self.near_right = copy(self.unit(1, 0), self.into(0, 0), self.ring(1))
            self.near_right.start()
            self.opp_left.wait_recv()
            self.add(self.unit(SIDE - 1, 1), self.opp.at[1])
            self.near_left = copy(self.unit(SIDE - 1, 1), self.into(1, 1), self.ring(SIDE - 1))
            self.near_left.start()

        def finish(self, dst):
            for made in (self.far_right, self.far_left, self.near_right, self.near_left):
                made.wait_recv()
            own = self.unit(0, None)
            dst[...] = (own[...].astype(F32) + self.main[0].astype(F32) + self.main[1].astype(F32)).astype(BF16)

    tile = min(256, count)

    def experts(start, rows):
        @pl.loop(0, rows // tile)
        def _(b):
            at = pl.ds(pl.multiple_of(start + b * tile, tile), tile)
            lhs = jnp.concatenate([x_all[i // SIDE, i % SIDE, at, :] for i in range(n_tp)], axis=1)
            pair = dot(lhs, wgu[...])
            hidden = silu_mul(pair[:, :LANES], pair[:, LANES:]).astype(BF16)
            for j in range(n_tp // 2):
                out = dot(hidden, wd[:, j * 2 * LANES:(j + 1) * 2 * LANES])
                for s in range(2):
                    i = 2 * j + s
                    part[i // SIDE, i % SIDE, at, :] = out[:, s * LANES:(s + 1) * LANES].astype(BF16)

    class Pair:
        def __init__(self, k):
            self.k = k
            self.a_start, self.b_start = 2 * k * count, (2 * k + 1) * count
            self.gathers = gather_pair((self.a_start, count), (self.b_start, count))
            one = (
                RingSum(lambda i, at: part.at[i, :, at], my, y_ring, opp1.at[0, k], main1.at[0, k], self.a_start),
                RingSum(lambda i, at: part.at[:, i, at], mx, x_ring, opp1.at[1, k], main1.at[1, k], self.b_start),
            )
            two = (
                RingSum(lambda i, at: q_a.at[k, i, at], mx, x_ring, opp2.at[0, k], main2.at[0, k], 0),
                RingSum(lambda i, at: q_b.at[k, i, at], my, y_ring, opp2.at[1, k], main2.at[1, k], 0),
            )
            self.sums = (one, two)

        def arrive(self):
            for chunk in (2 * self.k, 2 * self.k + 1):
                lo = cap if chunk == 0 else chunk * count
                got = x_all.at[my, mx, pl.ds(lo, (chunk + 1) * count - lo)]
                pltpu.make_async_copy(got, got, z_recv.at[chunk]).wait()

        def gather(self, phase, step):
            for g in self.gathers:
                getattr((g.one, g.two)[phase], step)()

        def compute(self):
            experts(self.a_start, 2 * count)

        def sum(self, phase, step):
            for s in self.sums[phase]:
                getattr(s, step)()

        def middle(self):
            self.sums[0][0].finish(q_a.at[self.k])
            self.sums[0][1].finish(q_b.at[self.k])

        def close(self):
            self.sums[1][0].finish(y_own.at[pl.ds(self.a_start, count)])
            self.sums[1][1].finish(y_own.at[pl.ds(self.b_start, count)])
            first = self.a_start // cap
            if first == 0:
                back[0:cap, :] = y_own[0:cap, :]

            @pl.loop(max(first, 1), first + 2 * count // cap)
            def _(i):
                at = pl.ds(pl.multiple_of(i * cap, cap), cap)
                pltpu.make_async_remote_copy(
                    src_ref=y_own.at[at], dst_ref=back.at[at], send_sem=zb_send, recv_sem=zb_recv,
                    device_id={"ep": peer_from(i), "tp": tp}, device_id_type=MESH,
                ).start()

    pairs = [Pair(k) for k in range(n_pairs)]
    last = n_pairs - 1

    for k, p in enumerate(pairs):
        p.arrive()
        p.gather(0, "start")
        p.gather(0, "relay")
        p.gather(0, "finish")
        p.gather(1, "start")
        if k == 0:
            shared_gather.two.relay()
            pool_gather.two.relay()
        else:
            pairs[k - 1].gather(1, "relay")
    for k, p in enumerate(pairs):
        if k == last:
            p.gather(1, "relay")
        p.gather(1, "finish")
        p.compute()
        p.sum(0, "start")
        if k > 0:
            pairs[k - 1].sum(0, "relay")
    for k, p in enumerate(pairs):
        if k == last:
            p.sum(0, "relay")
        p.middle()
        p.sum(1, "start")
        if k > 0:
            pairs[k - 1].sum(1, "relay")
            pairs[k - 1].close()
    pairs[last].sum(1, "relay")
    pairs[last].close()

    shared_gather.two.finish()
    pool_gather.two.finish()
    for name in ("po_a", "po_b", "sd"):
        loads[name].wait()
    lane = lax.broadcasted_iota(jnp.int32, (tok // 2, LANES), 1)
    zero = jnp.zeros((tok // 2, LANES), BF16)
    upper, lower = [], []
    for i in range(n_tp):
        block = x_all[i // SIDE, i % SIDE, pool_start:pool_start + tok // 2, :]
        upper.append(jnp.where(lane < narrow, block, zero))
        lower.append(jnp.where(lane < narrow, zero, block))
    lhs = jnp.concatenate([jnp.concatenate(upper, axis=1), jnp.concatenate(lower, axis=1)], axis=0)
    mix_out_ref[...] = dot(lhs, po2[...].reshape(2 * n_tp * narrow, LANES)).astype(BF16)
    lhs = jnp.concatenate([x_all[i // SIDE, i % SIDE, shared_rows, :] for i in range(n_tp)], axis=1)
    result = dot(lhs, sd[...])

    arrived = back.at[pl.ds(cap, rows_all - cap)]
    pltpu.make_async_copy(arrived, arrived, zb_recv).wait()
    over = (((0,), (0,)), ((), ()))
    result += lax.dot_general(chi[...], back[...], over, preferred_element_type=F32)
    result += lax.dot_general(clo[...], back[...], over, preferred_element_type=F32)
    moe_out_ref[...] = result.astype(BF16)

    for made in sent:
        made.wait_send()
    for whole, sem in ((outgoing, z_send), (y_own, zb_send)):
        gone = whole.at[pl.ds(cap, rows_all - cap)]
        pltpu.make_async_copy(gone, gone, sem).wait()
    pltpu.make_async_copy(sq_in, sq_in, sq_send).wait()


def on_device(n_pairs, mix_input, expert_input, mix_gain, moe_gain, pool_in, pool_scale, pool_gain, pool_out, route,
              route_score, expert_gate, expert_up, expert_down, shared_gate, shared_up, shared_down):
    n_ep, n_tp = lax.axis_size("ep"), lax.axis_size("tp")
    tok, width = mix_input.shape
    top = route.shape[1]
    cap = 2 * tok * top // n_ep
    rows = cap * n_ep
    narrow = pool_in.shape[1]
    count = rows // (2 * n_pairs)
    everything = rows + tok + tok // 2
    vmem = pl.BlockSpec(memory_space=pltpu.VMEM)
    hbm = pl.BlockSpec(memory_space=pltpu.HBM)
    dma = pltpu.SemaphoreType.DMA
    n_copies = 1 + 16 + n_pairs * 40
    return pl.pallas_call(
        functools.partial(kernel, n_pairs),
        out_shape=(
            jax.ShapeDtypeStruct((tok, pool_out.shape[1]), BF16),
            jax.ShapeDtypeStruct((tok, shared_down.shape[1]), BF16),
        ),
        in_specs=[vmem, hbm, vmem, vmem, hbm, vmem, vmem, hbm, vmem, vmem, hbm, hbm, hbm, hbm, hbm, hbm],
        out_specs=(vmem, vmem),
        scratch_shapes=[
            pltpu.VMEM((tok, width), BF16),
            pltpu.VMEM((width, 2 * LANES), BF16),
            pltpu.VMEM((LANES, width), BF16),
            pltpu.VMEM((width, 2 * LANES), BF16),
            pltpu.VMEM((width, LANES), BF16),
            pltpu.VMEM((width, narrow), BF16),
            pltpu.VMEM((n_tp, 2, narrow, LANES), BF16),
            pltpu.VMEM((tok, width), BF16),
            pltpu.VMEM((tok, width), BF16),
            pltpu.VMEM((rows, LANES), BF16),
            pltpu.VMEM((rows, LANES), BF16),
            pltpu.VMEM((rows, LANES), BF16),
            pltpu.VMEM((rows, LANES), BF16),
            pltpu.VMEM((SIDE, SIDE, everything, LANES), BF16),
            pltpu.VMEM((SIDE, SIDE, rows, LANES), BF16),
            pltpu.VMEM((n_pairs, SIDE, count, LANES), BF16),
            pltpu.VMEM((n_pairs, SIDE, count, LANES), BF16),
            pltpu.VMEM((rows, LANES), BF16),
            pltpu.VMEM((rows, LANES), BF16),
            pltpu.VMEM((2, n_pairs, 2, SIDE, count // 2, LANES), BF16),
            pltpu.VMEM((2, n_pairs, 2, SIDE, count, LANES), BF16),
            pltpu.VMEM((2, n_pairs, 2, count // 2, LANES), BF16),
            pltpu.VMEM((2, n_pairs, 2, count, LANES), BF16),
            pltpu.VMEM((16, LANES), BF16),
            pltpu.VMEM((16, LANES), BF16),
            pltpu.VMEM((8, LANES), F32),
            pltpu.VMEM((n_tp - 1, 8, LANES), F32),
            dma((10,)),
            dma((n_copies,)),
            dma((n_copies,)),
            dma,
            dma((2 * n_pairs,)),
            dma,
            dma,
            dma,
            dma,
        ],
        compiler_params=pltpu.CompilerParams(
            collective_id=0, has_side_effects=True, vmem_limit_bytes=60 * 1024 * 1024
        ),
    )(
        expert_input,
        mix_input,
        mix_gain.reshape(1, -1),
        moe_gain.reshape(1, -1),
        pool_in,
        pool_scale.reshape(1, -1),
        pool_gain.reshape(1, -1),
        pool_out.reshape(n_tp, narrow, pool_out.shape[1]),
        route,
        route_score,
        expert_gate,
        expert_up,
        expert_down,
        shared_gate,
        shared_up,
        shared_down,
    )


def solution(mesh):
    return jax.shard_map(
        functools.partial(on_device, 2),
        mesh=mesh,
        in_specs=(
            P("ep", None),
            P("ep", None),
            P(),
            P(),
            P(None, "tp"),
            P("tp"),
            P("tp"),
            P(None, "tp"),
            P("ep", None),
            P("ep", None),
            P("ep", None, "tp"),
            P("ep", None, "tp"),
            P("ep", "tp", None),
            P(None, "tp"),
            P(None, "tp"),
            P(None, "tp"),
        ),
        out_specs=(P("ep", "tp"), P("ep", "tp")),
        check_vma=False,
    )
```

```python
import functools
import math

import jax
import jax.numpy as jnp
from jax import lax
from jax.experimental import pallas as pl
from jax.experimental.pallas import tpu as pltpu
from jax.sharding import PartitionSpec as P

MESH = pl.DeviceIdType.MESH
F32, BF16 = jnp.float32, jnp.bfloat16
EPS = 1e-06
SIDE = 4
LANES = 128


def dot(a, b):
    return jnp.dot(a, b, preferred_element_type=F32)


def silu_mul(gate, upper):
    return gate / (1.0 + jnp.exp(-gate)) * upper


class Sems:
    def __init__(self, recv):
        self.recv, self.used = recv, 0

    def take(self):
        at = self.used
        self.used += 1
        return self.recv.at[at]


def kernel(
    n_pairs,
    xe_hbm, xm_hbm, mix_gain_ref, moe_gain_ref, pin_hbm, pscale_ref, pgain_ref, pout_hbm, route_ref, score_ref,
    eg_hbm, eu_hbm, ed_hbm, sg_hbm, su_hbm, sd_hbm,
    mix_out_ref, moe_out_ref,
    xe, xm, wgu, wd, sgu, sd, pin, po2, mn, mm, sel, chi, clo, outgoing, x_all, part, q_a, q_b, y_own, back,
    opp1, main1, opp2, main2, halo_out, halo_in, sq_out, sq_in,
    load_sems, send_sems, recv_sems, z_send, z_recv, zb_send, zb_recv, sq_send, sq_recv,
):
    n_ep, n_tp = lax.axis_size("ep"), lax.axis_size("tp")
    ep, tp = lax.axis_index("ep"), lax.axis_index("tp")
    n_z = n_ep // 2
    z, core = ep // 2, ep % 2
    my, mx = tp // SIDE, tp % SIDE
    tok, width = xe_hbm.shape
    rows_all = outgoing.shape[0]
    cap = rows_all // n_ep
    sems = Sems(recv_sems)

    def slot_place(i):
        pair, other = i // 2, i % 2
        far = (pair + 1) // 2
        step = jnp.where(pair % 2 == 1, far, n_z - far)
        return step, other

    def peer_to(i):
        step, other = slot_place(i)
        return ((z + step) % n_z) * 2 + (core + other) % 2

    def peer_from(i):
        step, other = slot_place(i)
        return ((z + n_z - step) % n_z) * 2 + (core + other) % 2

    loads = {}

    def load(name, src, dst):
        loads[name] = pltpu.make_async_copy(src, dst, load_sems.at[len(loads)])
        loads[name].start()

    load("xe", xe_hbm, xe)

    barrier = pltpu.get_barrier_semaphore()

    @pl.loop(1, n_ep)
    def _(i):
        pl.semaphore_signal(barrier, inc=1, device_id={"ep": (ep + i) % n_ep, "tp": tp}, device_id_type=MESH)

    @pl.loop(1, n_tp)
    def _(i):
        pl.semaphore_signal(barrier, inc=1, device_id={"ep": ep, "tp": (tp + i) % n_tp}, device_id_type=MESH)

    load("xm", xm_hbm, xm)
    load("pin", pin_hbm, pin)
    load("sg", sg_hbm, sgu.at[:, 0:LANES])
    load("su", su_hbm, sgu.at[:, LANES:2 * LANES])
    load("eg", eg_hbm.at[0], wgu.at[:, 0:LANES])
    load("eu", eu_hbm.at[0], wgu.at[:, LANES:2 * LANES])
    load("ed", ed_hbm.at[0], wd)
    load("po_a", pout_hbm, po2.at[:, 0])
    load("po_b", pout_hbm, po2.at[:, 1])
    load("sd", sd_hbm, sd)

    def row_norm(src, gain_ref, dst):
        @pl.loop(0, tok // 16)
        def _(b):
            at = pl.ds(pl.multiple_of(b * 16, 16), 16)
            values = src[at, :].astype(F32)
            scale = lax.rsqrt(jnp.mean(values * values, axis=-1, keepdims=True) + EPS)
            dst[at, :] = (values * scale * gain_ref[...]).astype(BF16)


    top = route_ref.shape[0]
    routes = [route_ref[k:k + 1, :].astype(F32) for k in range(top)]
    scores = [score_ref[k:k + 1, :] for k in range(top)]
    slot_i = lax.broadcasted_iota(jnp.int32, (n_ep, tok), 0)
    pair_i, other_i = slot_i // 2, slot_i % 2
    far_i = (pair_i + 1) // 2
    step_i = jnp.where(pair_i % 2 == 1, far_i, n_z - far_i)
    expert_i = (((z + step_i) % n_z) * 2 + (core + other_i) % 2).astype(F32)
    total = scores[0]
    for k in range(1, top):
        total = total + scores[k]
    hit = jnp.zeros((n_ep, tok), F32)
    weight = jnp.zeros((n_ep, tok), F32)
    for k in range(top):
        same = expert_i == routes[k]
        hit = jnp.where(same, 1.0, hit)
        weight = jnp.where(same, 2.5 * scores[k] / total, weight)
    before = (
        lax.broadcasted_iota(jnp.int32, (tok, tok), 0) < lax.broadcasted_iota(jnp.int32, (tok, tok), 1)
    )
    rank = dot(hit.astype(BF16), jnp.where(before, 1.0, 0.0).astype(BF16))
    place = jnp.where(hit > 0.0, rank, -1.0)
    slot_row = lax.broadcasted_iota(jnp.int32, (cap, tok), 0).astype(F32)
    for i in range(n_ep):
        sel[i * cap:(i + 1) * cap, :] = jnp.where(place[i:i + 1, :] == slot_row, 1.0, 0.0).astype(BF16)

    loads["xe"].wait()
    row_norm(xe, moe_gain_ref, mn)
    share = mn[:, pl.ds(pl.multiple_of(tp * LANES, LANES), LANES)]
    outgoing[...] = dot(sel[...], share).astype(BF16)
    x_all[my, mx, 0:cap, :] = outgoing[0:cap, :]

    pl.semaphore_wait(barrier, n_ep - 1 + n_tp - 1)

    near = n_pairs // 4
    order = list(range(near)) + list(range(2 * near, n_pairs)) + list(range(2 * near - 1, near - 1, -1))
    per_pair = n_ep // n_pairs
    for k in order:

        @pl.loop(max(1, k * per_pair), (k + 1) * per_pair)
        def _(i):
            at = pl.ds(pl.multiple_of(i * cap, cap), cap)
            pltpu.make_async_remote_copy(
                src_ref=outgoing.at[at], dst_ref=x_all.at[my, mx, at], send_sem=z_send, recv_sem=z_recv.at[k],
                device_id={"ep": peer_to(i), "tp": tp}, device_id_type=MESH,
            ).start()

    def copy(src, dst, where, group):
        send_all[group] += math.prod(src.shape)
        return pltpu.make_async_remote_copy(
            src_ref=src, dst_ref=dst, send_sem=send_sems.at[group], recv_sem=sems.take(),
            device_id=where, device_id_type=MESH,
        )

    send_all = [0] * (n_pairs + 3)
    x_ring = lambda step: {"ep": ep, "tp": my * SIDE + (mx + step) % SIDE}
    y_ring = lambda step: {"ep": ep, "tp": ((my + step) % SIDE) * SIDE + mx}

    class Ring:
        def __init__(self, view, me, ring, start, count, group):
            self.view, self.me, self.ring, self.start_row, self.count = view, me, ring, start, count
            self.group = group

        def unit(self, step, part=None):
            half = self.count // 2
            lo, n = {None: (0, self.count), 0: (0, half), 1: (half, half)}[part]
            return self.view((self.me + step) % SIDE, pl.ds(self.start_row + lo, n))

        def start(self):
            own = self.unit(0)
            self.right = copy(own, own, self.ring(1), self.group)
            self.left = copy(own, own, self.ring(SIDE - 1), self.group)
            self.right.start()
            self.left.start()

        def relay(self):
            first, second = self.unit(SIDE - 1, 0), self.unit(1, 1)
            self.right.wait_recv()
            self.on_right = copy(first, first, self.ring(1), self.group)
            self.on_right.start()
            self.left.wait_recv()
            self.on_left = copy(second, second, self.ring(SIDE - 1), self.group)
            self.on_left.start()

        def finish(self):
            self.on_right.wait_recv()
            self.on_left.wait_recv()

    class Gather:
        def __init__(self, start, count, group, x_first):
            along_x = lambda i, at: x_all.at[my, i, at]
            along_y = lambda i, at: x_all.at[i, mx, at]
            whole_y = lambda i, at: x_all.at[i, :, at]
            whole_x = lambda i, at: x_all.at[:, i, at]
            if x_first:
                self.one = Ring(along_x, mx, x_ring, start, count, group)
                self.two = Ring(whole_y, my, y_ring, start, count, group)
            else:
                self.one = Ring(along_y, my, y_ring, start, count, group)
                self.two = Ring(whole_x, mx, x_ring, start, count, group)

    class Rows:
        def __init__(self, start, count, group):
            self.gathers = Gather(start, count // 2, group, True), Gather(start + count // 2, count // 2, group, False)

        def arrive(self):
            pass

        def gather(self, phase, step):
            for g in self.gathers:
                getattr((g.one, g.two)[phase], step)()


    loads["xm"].wait()
    row_norm(xm, mix_gain_ref, mm)
    loads["pin"].wait()
    narrow = pin.shape[0]
    pooled_in = lax.dot_general(mm[...], pin[...], (((1,), (1,)), ((), ())), preferred_element_type=F32)
    pooled_in = jnp.concatenate([pooled_in, jnp.zeros((tok, LANES - narrow), F32)], axis=1).astype(BF16)
    halo_out[...] = pooled_in[tok - 16:, :]
    halo = copy(halo_out, halo_in, {"ep": (ep + 1) % n_ep, "tp": tp}, len(send_all) - 1)
    halo.start()

    loads["sg"].wait()
    loads["su"].wait()
    both = dot(mn[...], sgu[...])
    shared_rows = slice(rows_all, rows_all + tok)
    x_all[my, mx, shared_rows, :] = silu_mul(both[:, :LANES], both[:, LANES:]).astype(BF16)

    def windows():
        halo.wait_recv()
        carried = jnp.where(ep > 0, halo_in[...].astype(F32), 0.0)
        ext = jnp.concatenate([carried, pooled_in.astype(F32)], axis=0)
        sums, chosen, window = ext, None, 1
        for index in range(4):
            sums = sums + pltpu.roll(sums, window, 0)
            window *= 2
            chosen = sums if chosen is None else jnp.where(my >= index, sums, chosen)
        position = (ep * tok + lax.broadcasted_iota(jnp.int32, (tok, LANES), 0) + 1).astype(F32)
        widest = lax.shift_left(2, my).astype(F32)
        zeros_right = jnp.zeros((1, LANES - narrow), F32)
        pscale = jnp.concatenate([pscale_ref[...], zeros_right], axis=1)
        pgain = jnp.concatenate([pgain_ref[...], zeros_right], axis=1)
        scaled = (chosen[16:, :] / jnp.minimum(position, widest) - pooled_in.astype(F32)) * pscale
        squares = jnp.sum(scaled * scaled, axis=1, keepdims=True)
        squares = jnp.broadcast_to(squares, (tok, LANES)).T[0:8, :]
        sq_out[...] = squares

        @pl.loop(1, n_tp)
        def _(i):
            pltpu.make_async_remote_copy(
                src_ref=sq_out, dst_ref=sq_in.at[i - 1], send_sem=sq_send, recv_sem=sq_recv,
                device_id={"ep": ep, "tp": (tp + i) % n_tp}, device_id_type=MESH,
            ).start()
        return scaled, squares, pgain

    def combine_terms():
        high = weight.astype(BF16).astype(F32)
        low = weight - high
        for i in range(n_ep):
            at = slice(i * cap, (i + 1) * cap)
            same = place[i:i + 1, :] == slot_row
            chi[at, :] = jnp.where(same, high[i:i + 1, :], 0.0).astype(BF16)
            clo[at, :] = jnp.where(same, low[i:i + 1, :], 0.0).astype(BF16)

    pool_start = rows_all + tok

    def pool_norm(scaled, squares, pgain):
        pltpu.make_async_copy(sq_in, sq_in, sq_recv).wait()
        total = squares
        for i in range(n_tp - 1):
            total = total + sq_in[i]
        total = jnp.broadcast_to(total[0:1, :], (tok, LANES)).T
        pooled = (scaled * lax.rsqrt(total / (narrow * n_tp) + EPS) * pgain).astype(BF16).astype(F32)
        packed = pooled[:tok // 2, :] + pltpu.roll(pooled[tok // 2:, :], narrow, 1)
        x_all[my, mx, pool_start:pool_start + tok // 2, :] = packed.astype(BF16)

    count = rows_all // (2 * n_pairs)
    half = count // 2

    class RingSum:
        def __init__(self, view, me, ring, opp, main, start, group):
            self.view, self.me, self.ring, self.opp, self.main, self.start_row = view, me, ring, opp, main, start
            self.group = group

        def unit(self, step, part):
            lo, n = {None: (0, count), 0: (0, half), 1: (half, half)}[part]
            return self.view((self.me + step) % SIDE, pl.ds(self.start_row + lo, n))

        def into(self, side, part):
            at = pl.ds(part * half, half)
            return self.main.at[(side,) + (slice(None),) * (len(self.main.shape) - 3) + (at,)]

        def start(self):
            self.opp_right = copy(self.unit(2, 0), self.opp.at[0], self.ring(1), self.group)
            self.opp_left = copy(self.unit(2, 1), self.opp.at[1], self.ring(SIDE - 1), self.group)
            self.far_right = copy(self.unit(1, 1), self.into(0, 1), self.ring(1), self.group)
            self.far_left = copy(self.unit(SIDE - 1, 0), self.into(1, 0), self.ring(SIDE - 1), self.group)
            for made in (self.opp_right, self.opp_left, self.far_right, self.far_left):
                made.start()

        def add(self, unit, extra):
            unit[...] = (unit[...].astype(F32) + extra[...].astype(F32)).astype(BF16)

        def relay(self):
            self.opp_right.wait_recv()
            self.add(self.unit(1, 0), self.opp.at[0])
            self.near_right = copy(self.unit(1, 0), self.into(0, 0), self.ring(1), self.group)
            self.near_right.start()
            self.opp_left.wait_recv()
            self.add(self.unit(SIDE - 1, 1), self.opp.at[1])
            self.near_left = copy(self.unit(SIDE - 1, 1), self.into(1, 1), self.ring(SIDE - 1), self.group)
            self.near_left.start()

        def finish(self, dst):
            for made in (self.far_right, self.far_left, self.near_right, self.near_left):
                made.wait_recv()
            own = self.unit(0, None)
            dst[...] = (own[...].astype(F32) + self.main[0].astype(F32) + self.main[1].astype(F32)).astype(BF16)

    tile = min(256, count)

    def experts(start, rows):
        @pl.loop(0, rows // tile)
        def _(b):
            at = pl.ds(pl.multiple_of(start + b * tile, tile), tile)
            lhs = jnp.concatenate([x_all[i // SIDE, i % SIDE, at, :] for i in range(n_tp)], axis=1)
            pair = dot(lhs, wgu[...])
            hidden = silu_mul(pair[:, :LANES], pair[:, LANES:]).astype(BF16)
            for j in range(n_tp // 2):
                out = dot(hidden, wd[:, j * 2 * LANES:(j + 1) * 2 * LANES])
                for s in range(2):
                    i = 2 * j + s
                    part[i // SIDE, i % SIDE, at, :] = out[:, s * LANES:(s + 1) * LANES].astype(BF16)

    class Pair(Rows):
        def __init__(self, k):
            self.k = k
            self.a_start, self.b_start = 2 * k * count, (2 * k + 1) * count
            super().__init__(self.a_start, 2 * count, k)
            one = (
                RingSum(lambda i, at: part.at[i, :, at], my, y_ring, opp1.at[0, k], main1.at[0, k], self.a_start, k),
                RingSum(lambda i, at: part.at[:, i, at], mx, x_ring, opp1.at[1, k], main1.at[1, k], self.b_start, k),
            )
            two = (
                RingSum(lambda i, at: q_a.at[k, i, at], mx, x_ring, opp2.at[0, k], main2.at[0, k], 0, k),
                RingSum(lambda i, at: q_b.at[k, i, at], my, y_ring, opp2.at[1, k], main2.at[1, k], 0, k),
            )
            self.sums = (one, two)

        def arrive(self):
            lo = max(cap, self.a_start)
            got = x_all.at[my, mx, pl.ds(lo, self.a_start + 2 * count - lo)]
            pltpu.make_async_copy(got, got, z_recv.at[self.k]).wait()

        def compute(self):
            if self is pairs[0]:
                for name in ("eg", "eu", "ed"):
                    loads[name].wait()
            experts(self.a_start, 2 * count)

        def sum(self, phase, step):
            for s in self.sums[phase]:
                getattr(s, step)()

        def middle(self):
            self.sums[0][0].finish(q_a.at[self.k])
            self.sums[0][1].finish(q_b.at[self.k])

        def close(self):
            self.sums[1][0].finish(y_own.at[pl.ds(self.a_start, count)])
            self.sums[1][1].finish(y_own.at[pl.ds(self.b_start, count)])
            first = self.a_start // cap
            if first == 0:
                back[0:cap, :] = y_own[0:cap, :]

            @pl.loop(max(first, 1), first + 2 * count // cap)
            def _(i):
                at = pl.ds(pl.multiple_of(i * cap, cap), cap)
                pltpu.make_async_remote_copy(
                    src_ref=y_own.at[at], dst_ref=back.at[at], send_sem=zb_send, recv_sem=zb_recv.at[self.k],
                    device_id={"ep": peer_from(i), "tp": tp}, device_id_type=MESH,
                ).start()

    pairs = [Pair(k) for k in order]

    def plain_outputs():
        items[0].gather(1, "finish")
        items[-1].gather(1, "finish")
        for name in ("po_a", "po_b", "sd"):
            loads[name].wait()
        lane = lax.broadcasted_iota(jnp.int32, (tok // 2, LANES), 1)
        zero = jnp.zeros((tok // 2, LANES), BF16)
        upper, lower = [], []
        for i in range(n_tp):
            block = x_all[i // SIDE, i % SIDE, pool_start:pool_start + tok // 2, :]
            upper.append(jnp.where(lane < narrow, block, zero))
            lower.append(jnp.where(lane < narrow, zero, block))
        lhs = jnp.concatenate([jnp.concatenate(upper, axis=1), jnp.concatenate(lower, axis=1)], axis=0)
        mix_out_ref[...] = dot(lhs, po2[...].reshape(2 * n_tp * narrow, LANES)).astype(BF16)
        lhs = jnp.concatenate([x_all[i // SIDE, i % SIDE, shared_rows, :] for i in range(n_tp)], axis=1)
        result = dot(lhs, sd[...])
        return result

    items = [Rows(rows_all, tok, n_pairs)] + pairs + [Rows(pool_start, tok // 2, n_pairs + 1)]

    def gathered(index):
        return items[index] if 0 <= index < len(items) else None

    def summed(index):
        return pairs[index - 1] if 1 <= index <= n_pairs else None

    for s in range(n_pairs + 9):
        if s == 5:
            pool_norm(*pool_state)
        if p := gathered(s):
            p.arrive()
            p.gather(0, "start")
        if p := gathered(s - 1):
            p.gather(0, "relay")
        if p := gathered(s - 2):
            p.gather(0, "finish")
            p.gather(1, "start")
        if p := gathered(s - 3):
            p.gather(1, "relay")
        if p := summed(s - 4):
            p.gather(1, "finish")
            p.compute()
            p.sum(0, "start")
        if s == 1:
            pool_state = windows()
        if s == 2:
            combine_terms()
        if p := summed(s - 5):
            p.sum(0, "relay")
        if p := summed(s - 6):
            p.middle()
            p.sum(1, "start")
        if s == n_pairs + 6:
            result = plain_outputs()
        if p := summed(s - 7):
            p.sum(1, "relay")
        if p := summed(s - 8):
            p.close()

    over = (((0,), (0,)), ((), ()))
    for p in pairs:
        lo = max(cap, p.a_start)
        arrived = back.at[pl.ds(lo, p.a_start + 2 * count - lo)]
        pltpu.make_async_copy(arrived, arrived, zb_recv.at[p.k]).wait()
        at = slice(p.a_start, p.a_start + 2 * count)
        result += lax.dot_general(chi[at, :], back[at, :], over, preferred_element_type=F32)
        result += lax.dot_general(clo[at, :], back[at, :], over, preferred_element_type=F32)
    moe_out_ref[...] = result.astype(BF16)

    for group, size in enumerate(send_all):
        blocks = size // (60 * 16 * LANES)
        gone = halo_out if blocks == 0 else part.at[0, 0:blocks, 0:60 * 16]
        pltpu.make_async_copy(gone, gone, send_sems.at[group]).wait()
    for whole, sem in ((outgoing, z_send), (y_own, zb_send)):
        gone = whole.at[pl.ds(cap, rows_all - cap)]
        pltpu.make_async_copy(gone, gone, sem).wait()
    pltpu.make_async_copy(sq_in, sq_in, sq_send).wait()


def on_device(n_pairs, mix_input, expert_input, mix_gain, moe_gain, pool_in, pool_scale, pool_gain, pool_out, route,
              route_score, expert_gate, expert_up, expert_down, shared_gate, shared_up, shared_down):
    n_ep, n_tp = lax.axis_size("ep"), lax.axis_size("tp")
    tok, width = mix_input.shape
    top = route.shape[1]
    cap = 2 * tok * top // n_ep
    rows = cap * n_ep
    narrow = pool_in.shape[1]
    count = rows // (2 * n_pairs)
    everything = rows + tok + tok // 2
    vmem = pl.BlockSpec(memory_space=pltpu.VMEM)
    hbm = pl.BlockSpec(memory_space=pltpu.HBM)
    dma = pltpu.SemaphoreType.DMA
    n_copies = 1 + 32 + n_pairs * 40
    return pl.pallas_call(
        functools.partial(kernel, n_pairs),
        out_shape=(
            jax.ShapeDtypeStruct((tok, pool_out.shape[1]), BF16),
            jax.ShapeDtypeStruct((tok, shared_down.shape[1]), BF16),
        ),
        in_specs=[hbm, hbm, vmem, vmem, hbm, vmem, vmem, hbm, vmem, vmem, hbm, hbm, hbm, hbm, hbm, hbm],
        out_specs=(vmem, vmem),
        scratch_shapes=[
            pltpu.VMEM((tok, width), BF16),
            pltpu.VMEM((tok, width), BF16),
            pltpu.VMEM((width, 2 * LANES), BF16),
            pltpu.VMEM((LANES, width), BF16),
            pltpu.VMEM((width, 2 * LANES), BF16),
            pltpu.VMEM((width, LANES), BF16),
            pltpu.VMEM((narrow, width), BF16),
            pltpu.VMEM((n_tp, 2, narrow, LANES), BF16),
            pltpu.VMEM((tok, width), BF16),
            pltpu.VMEM((tok, width), BF16),
            pltpu.VMEM((rows, LANES), BF16),
            pltpu.VMEM((rows, LANES), BF16),
            pltpu.VMEM((rows, LANES), BF16),
            pltpu.VMEM((rows, LANES), BF16),
            pltpu.VMEM((SIDE, SIDE, everything, LANES), BF16),
            pltpu.VMEM((SIDE, SIDE, rows, LANES), BF16),
            pltpu.VMEM((n_pairs, SIDE, count, LANES), BF16),
            pltpu.VMEM((n_pairs, SIDE, count, LANES), BF16),
            pltpu.VMEM((rows, LANES), BF16),
            pltpu.VMEM((rows, LANES), BF16),
            pltpu.VMEM((2, n_pairs, 2, SIDE, count // 2, LANES), BF16),
            pltpu.VMEM((2, n_pairs, 2, SIDE, count, LANES), BF16),
            pltpu.VMEM((2, n_pairs, 2, count // 2, LANES), BF16),
            pltpu.VMEM((2, n_pairs, 2, count, LANES), BF16),
            pltpu.VMEM((16, LANES), BF16),
            pltpu.VMEM((16, LANES), BF16),
            pltpu.VMEM((8, LANES), F32),
            pltpu.VMEM((n_tp - 1, 8, LANES), F32),
            dma((11,)),
            dma((n_pairs + 3,)),
            dma((n_copies,)),
            dma,
            dma((n_pairs,)),
            dma,
            dma((n_pairs,)),
            dma,
            dma,
        ],
        compiler_params=pltpu.CompilerParams(
            collective_id=0, has_side_effects=True, vmem_limit_bytes=60 * 1024 * 1024
        ),
    )(
        expert_input,
        mix_input,
        mix_gain.reshape(1, -1),
        moe_gain.reshape(1, -1),
        pool_in.T,
        pool_scale.reshape(1, -1),
        pool_gain.reshape(1, -1),
        pool_out.reshape(n_tp, narrow, pool_out.shape[1]),
        route.T,
        route_score.T,
        expert_gate,
        expert_up,
        expert_down,
        shared_gate,
        shared_up,
        shared_down,
    )


def solution(mesh):
    return jax.shard_map(
        functools.partial(on_device, 8),
        mesh=mesh,
        in_specs=(
            P("ep", None),
            P("ep", None),
            P(),
            P(),
            P(None, "tp"),
            P("tp"),
            P("tp"),
            P(None, "tp"),
            P("ep", None),
            P("ep", None),
            P("ep", None, "tp"),
            P("ep", None, "tp"),
            P("ep", "tp", None),
            P(None, "tp"),
            P(None, "tp"),
            P(None, "tp"),
        ),
        out_specs=(P("ep", "tp"), P("ep", "tp")),
        check_vma=False,
    )
```

```python
import functools

import jax
import jax.numpy as jnp
from jax import lax
from jax.experimental import pallas as pl
from jax.experimental.pallas import tpu as pltpu
from jax.sharding import PartitionSpec as P

MESH = pl.DeviceIdType.MESH
F32, BF16 = jnp.float32, jnp.bfloat16
EPS = 1e-06
SIDE = 4
DISPATCH_TICK, WINDOW_TICK, POOL_TICK = 1, 8, 14
LAGS = {"relay": 2, "along": 4, "along_relay": 6, "compute": 8, "first_relay": 10, "second": 12, "second_relay": 14, "close": 16}
LANES = 128


def dot(a, b):
    return jnp.dot(a, b, preferred_element_type=F32)


def silu_mul(gate, upper):
    return gate / (1.0 + jnp.exp(-gate)) * upper


def kernel(
    n_pairs,
    xe_hbm, xm_hbm, mix_gain_ref, moe_gain_ref, pin_hbm, pscale_ref, pgain_ref, pout_hbm, route_ref, score_ref,
    eg_hbm, eu_hbm, ed_hbm, sg_hbm, su_hbm, sd_hbm,
    out_ref,
    xe, xm, wgu, wd, sgu, sd, pin, po2, mn, mm, sel, chi, clo, outgoing, x_all, part, q_a, q_b, y_own, back,
    opp1, main1, opp2, main2, halo_out, halo_in, sq_out, sq_in,
    load_sems, send_sems, recv_sems, rows_sems, z_send, z_recv, zb_send, zb_recv, sq_send, sq_recv,
):
    n_ep, n_tp = lax.axis_size("ep"), lax.axis_size("tp")
    ep, tp = lax.axis_index("ep"), lax.axis_index("tp")
    n_z = n_ep // 2
    z, core = ep // 2, ep % 2
    my, mx = tp // SIDE, tp % SIDE
    tok, width = xe_hbm.shape
    rows_all = outgoing.shape[0]
    cap = rows_all // n_ep

    def wrap(value, size):
        return lax.rem(value, size)

    z_bits = [wrap(z // 2 ** b, 2) for b in range(8) if 2 ** b < n_z]
    late = z // (n_z // 2)

    def peer(i):
        other = z
        for b, bit in enumerate(z_bits):
            if i // 2 // 2 ** b % 2:
                other = other + 2 ** b * (1 - 2 * bit)
        return other * 2 + wrap(core + i % 2, 2)

    def by_half(low, high):
        return low if isinstance(low, int) and low == high else low + late * (high - low)

    loads = {}

    def load(name, src, dst):
        loads[name] = pltpu.make_async_copy(src, dst, load_sems.at[len(loads)])
        loads[name].start()

    load("xe", xe_hbm, xe)

    barrier = pltpu.get_barrier_semaphore()
    for i in range(n_ep - 1, 0, -1):
        pl.semaphore_signal(barrier, inc=1, device_id={"ep": peer(i), "tp": tp}, device_id_type=MESH)
    for i in range(1, n_tp):
        pl.semaphore_signal(barrier, inc=1, device_id={"ep": ep, "tp": wrap(tp + i, n_tp)}, device_id_type=MESH)

    load("xm", xm_hbm, xm)
    load("pin", pin_hbm, pin)
    load("sg", sg_hbm, sgu.at[:, 0:LANES])
    load("su", su_hbm, sgu.at[:, LANES:2 * LANES])
    load("eg", eg_hbm.at[0], wgu.at[:, 0:LANES])
    load("eu", eu_hbm.at[0], wgu.at[:, LANES:2 * LANES])
    load("ed", ed_hbm.at[0], wd)
    load("po_a", pout_hbm, po2.at[:, 0])
    load("po_b", pout_hbm, po2.at[:, 1])
    load("sd", sd_hbm, sd)

    def row_norm(src, gain_ref, dst):
        for b in range(tok // 16):
            at = slice(b * 16, (b + 1) * 16)
            values = src[at, :].astype(F32)
            scale = lax.rsqrt(jnp.mean(values * values, axis=-1, keepdims=True) + EPS)
            dst[at, :] = (values * scale * gain_ref[...]).astype(BF16)


    top = route_ref.shape[0]
    routes = [route_ref[k:k + 1, :].astype(F32) for k in range(top)]
    scores = [score_ref[k:k + 1, :] for k in range(top)]
    slot_i = lax.broadcasted_iota(jnp.int32, (n_ep, tok), 0)
    expert_i = (((slot_i // 2) ^ z) * 2 + ((slot_i % 2) ^ core)).astype(F32)
    total = scores[0]
    for k in range(1, top):
        total = total + scores[k]
    hit = jnp.zeros((n_ep, tok), F32)
    weight = jnp.zeros((n_ep, tok), F32)
    for k in range(top):
        same = expert_i == routes[k]
        hit = jnp.where(same, 1.0, hit)
        weight = jnp.where(same, 2.5 * scores[k] / total, weight)
    before = (
        lax.broadcasted_iota(jnp.int32, (tok, tok), 0) < lax.broadcasted_iota(jnp.int32, (tok, tok), 1)
    )
    rank = dot(hit.astype(BF16), jnp.where(before, 1.0, 0.0).astype(BF16))
    place = jnp.where(hit > 0.0, rank, -1.0)
    slot_row = lax.broadcasted_iota(jnp.int32, (cap, tok), 0).astype(F32)
    for i in range(n_ep):
        sel[i * cap:(i + 1) * cap, :] = jnp.where(place[i:i + 1, :] == slot_row, 1.0, 0.0).astype(BF16)

    loads["xe"].wait()
    row_norm(xe, moe_gain_ref, mn)
    share = mn[:, pl.ds(pl.multiple_of(tp * LANES, LANES), LANES)]
    outgoing[...] = dot(sel[...], share).astype(BF16)
    x_all[my, mx, 0:cap, :] = outgoing[0:cap, :]

    loads["sg"].wait()
    loads["su"].wait()
    both = dot(mn[...], sgu[...])
    shared_rows = slice(rows_all, rows_all + tok)
    x_all[my, mx, shared_rows, :] = silu_mul(both[:, :LANES], both[:, LANES:]).astype(BF16)

    pl.semaphore_wait(barrier, n_ep - 1 + n_tp - 1)

    middle, quarter = n_pairs // 2, n_pairs // 4
    low_order = list(range(n_pairs - 2)) + [n_pairs - 1, n_pairs - 2]
    high_order = list(range(quarter)) + list(range(middle, n_pairs)) + list(range(middle - 1, quarter - 1, -1))
    per_pair = n_ep // n_pairs

    def dispatch(chunks):
        for i in [i for k in chunks for i in range(max(1, k * per_pair), (k + 1) * per_pair)]:
            at = pl.ds(i * cap, cap)
            pltpu.make_async_remote_copy(
                src_ref=outgoing.at[at], dst_ref=x_all.at[my, mx, at], send_sem=z_send,
                recv_sem=z_recv.at[i // per_pair], device_id={"ep": peer(i), "tp": tp}, device_id_type=MESH,
            ).start()

    dispatch(range(quarter))

    x_ring = lambda step: {"ep": ep, "tp": my * SIDE + wrap(mx + step, SIDE)}
    y_ring = lambda step: {"ep": ep, "tp": wrap(my + step, SIDE) * SIDE + mx}

    def send_of(group):
        return send_sems.at[group // quarter if group < n_pairs else 4 + group - n_pairs]

    def recv_of(group, stage):
        return recv_sems.at[group, stage] if group < n_pairs else rows_sems.at[group - n_pairs, stage]

    def launch(group, stage, src, dst, where):
        pltpu.make_async_remote_copy(
            src_ref=src, dst_ref=dst, send_sem=send_of(group), recv_sem=recv_of(group, stage),
            device_id=where, device_id_type=MESH,
        ).start()

    def await_rows(sem, units, rows):
        spot = {2: part.at[0, 0:2, 0:rows], 4: part.at[0, :, 0:rows], 8: part.at[0:2, :, 0:rows],
                16: part.at[:, :, 0:rows]}[units]
        pltpu.make_async_copy(spot, spot, sem).wait()

    class Ring:
        def __init__(self, view, me, ring, start, count):
            self.view, self.me, self.ring, self.start_row, self.count = view, me, ring, start, count

        def unit(self, step, half=None):
            lo, n = (0, self.count) if half is None else (half * self.count // 2, self.count // 2)
            return self.view(wrap(self.me + step, SIDE), pl.ds(self.start_row + lo, n))

        def own(self, group, stage):
            unit = self.unit(0)
            launch(group, stage, unit, unit, self.ring(1))
            launch(group, stage, unit, unit, self.ring(SIDE - 1))

        def onward(self, group, stage):
            first, second = self.unit(SIDE - 1, 0), self.unit(1, 1)
            launch(group, stage, first, first, self.ring(1))
            launch(group, stage, second, second, self.ring(SIDE - 1))

    class Rows:
        def __init__(self, start, rows, group):
            self.group, self.count = group, rows // 2
            a, b = (start, self.count), (start + self.count, self.count)
            self.rings = (
                (
                    Ring(lambda i, at: x_all.at[my, i, at], mx, x_ring, *a),
                    Ring(lambda i, at: x_all.at[i, mx, at], my, y_ring, *b),
                ),
                (
                    Ring(lambda i, at: x_all.at[i, :, at], my, y_ring, *a),
                    Ring(lambda i, at: x_all.at[:, i, at], mx, x_ring, *b),
                ),
            )

        def arrive(self):
            pass

        def gather_start(self, phase):
            for ring in self.rings[phase]:
                ring.own(self.group, 2 * phase)

        def gather_relay(self, phase):
            await_rows(recv_of(self.group, 2 * phase), (4, 16)[phase], self.count)
            for ring in self.rings[phase]:
                ring.onward(self.group, 2 * phase + 1)

        def gather_finish(self, phase):
            await_rows(recv_of(self.group, 2 * phase + 1), (2, 8)[phase], self.count)

    narrow = pin.shape[0]

    def mix_local():
        loads["xm"].wait()
        row_norm(xm, mix_gain_ref, mm)
        loads["pin"].wait()
        pooled_in = lax.dot_general(mm[...], pin[...], (((1,), (1,)), ((), ())), preferred_element_type=F32)
        pooled_in = jnp.concatenate([pooled_in, jnp.zeros((tok, LANES - narrow), F32)], axis=1).astype(BF16)
        halo_out[...] = pooled_in[tok - 16:, :]
        halo = pltpu.make_async_remote_copy(
            src_ref=halo_out, dst_ref=halo_in, send_sem=sq_send.at[1], recv_sem=sq_recv.at[1],
            device_id={"ep": wrap(ep + 1, n_ep), "tp": tp}, device_id_type=MESH,
        )
        halo.start()
        return pooled_in, halo

    def windows(pooled_in, halo):
        halo.wait_recv()
        carried = jnp.where(ep > 0, halo_in[...].astype(F32), 0.0)
        ext = jnp.concatenate([carried, pooled_in.astype(F32)], axis=0)
        sums, chosen, window = ext, None, 1
        for index in range(4):
            sums = sums + pltpu.roll(sums, window, 0)
            window *= 2
            chosen = sums if chosen is None else jnp.where(my >= index, sums, chosen)
        position = (ep * tok + lax.broadcasted_iota(jnp.int32, (tok, LANES), 0) + 1).astype(F32)
        widest = lax.shift_left(2, my).astype(F32)
        zeros_right = jnp.zeros((1, LANES - narrow), F32)
        pscale = jnp.concatenate([pscale_ref[...], zeros_right], axis=1)
        pgain = jnp.concatenate([pgain_ref[...], zeros_right], axis=1)
        scaled = (chosen[16:, :] / jnp.minimum(position, widest) - pooled_in.astype(F32)) * pscale
        squares = jnp.sum(scaled * scaled, axis=1, keepdims=True)
        squares = jnp.broadcast_to(squares, (tok, LANES)).T[0:8, :]
        sq_out[...] = squares

        for i in range(1, n_tp):
            pltpu.make_async_remote_copy(
                src_ref=sq_out, dst_ref=sq_in.at[i - 1], send_sem=sq_send.at[0], recv_sem=sq_recv.at[0],
                device_id={"ep": ep, "tp": wrap(tp + i, n_tp)}, device_id_type=MESH,
            ).start()
        return scaled, squares, pgain

    def combine_terms():
        high = weight.astype(BF16).astype(F32)
        low = weight - high
        for i in range(n_ep):
            at = slice(i * cap, (i + 1) * cap)
            same = place[i:i + 1, :] == slot_row
            chi[at, :] = jnp.where(same, high[i:i + 1, :], 0.0).astype(BF16)
            clo[at, :] = jnp.where(same, low[i:i + 1, :], 0.0).astype(BF16)

    pool_start = rows_all + tok

    def pool_norm(scaled, squares, pgain):
        pltpu.make_async_copy(sq_in, sq_in, sq_recv.at[0]).wait()
        total = squares
        for i in range(n_tp - 1):
            total = total + sq_in[i]
        total = jnp.broadcast_to(total[0:1, :], (tok, LANES)).T
        pooled = (scaled * lax.rsqrt(total / (narrow * n_tp) + EPS) * pgain).astype(BF16).astype(F32)
        packed = pooled[:tok // 2, :] + pltpu.roll(pooled[tok // 2:, :], narrow, 1)
        x_all[my, mx, pool_start:pool_start + tok // 2, :] = packed.astype(BF16)

    count = rows_all // (2 * n_pairs)
    half = count // 2

    class RingSum:
        def __init__(self, view, me, ring, opp, main, start):
            self.view, self.me, self.ring, self.opp, self.main, self.start_row = view, me, ring, opp, main, start

        def unit(self, step, which=None):
            lo, n = (0, count) if which is None else (which * half, half)
            return self.view(wrap(self.me + step, SIDE), pl.ds(self.start_row + lo, n))

        def into(self, side, which):
            at = pl.ds(which * half, half)
            return self.main.at[(side,) + (slice(None),) * (len(self.main.shape) - 3) + (at,)]

        def across(self, group, stage):
            launch(group, stage, self.unit(2, 0), self.opp.at[0], self.ring(1))
            launch(group, stage, self.unit(2, 1), self.opp.at[1], self.ring(SIDE - 1))

        def plain(self, group, stage):
            launch(group, stage, self.unit(1, 1), self.into(0, 1), self.ring(1))
            launch(group, stage, self.unit(SIDE - 1, 0), self.into(1, 0), self.ring(SIDE - 1))

        def added(self, group, stage):
            for unit, extra, dst, where in (
                (self.unit(1, 0), self.opp.at[0], self.into(0, 0), self.ring(1)),
                (self.unit(SIDE - 1, 1), self.opp.at[1], self.into(1, 1), self.ring(SIDE - 1)),
            ):
                unit[...] = (unit[...].astype(F32) + extra[...].astype(F32)).astype(BF16)
                launch(group, stage, unit, dst, where)

        def total(self, dst):
            own = self.unit(0)
            dst[...] = (own[...].astype(F32) + self.main[0].astype(F32) + self.main[1].astype(F32)).astype(BF16)

    tile = min(256, 2 * count)

    def experts(start, rows):
        @pl.loop(0, rows // tile)
        def _(b):
            at = pl.ds(pl.multiple_of(start + b * tile, tile), tile)
            lhs = jnp.concatenate([x_all[i // SIDE, i % SIDE, at, :] for i in range(n_tp)], axis=1)
            pair = dot(lhs, wgu[...])
            hidden = silu_mul(pair[:, :LANES], pair[:, LANES:]).astype(BF16)
            for j in range(n_tp // 2):
                out = dot(hidden, wd[:, j * 2 * LANES:(j + 1) * 2 * LANES])
                for s in range(2):
                    i = 2 * j + s
                    part[i // SIDE, i % SIDE, at, :] = out[:, s * LANES:(s + 1) * LANES].astype(BF16)

    class Pair(Rows):
        def __init__(self, k):
            self.k, self.chunks = k, (low_order[k], high_order[k])
            self.chunk = by_half(*self.chunks)
            self.start = self.chunk * (2 * count)
            if k > 0:
                self.start = pl.multiple_of(self.start, 2 * count)
            super().__init__(self.start, 2 * count, k)
            self.sums = (
                (
                    RingSum(lambda i, at: part.at[i, :, at], my, y_ring, opp1.at[0, k], main1.at[0, k], self.start),
                    RingSum(
                        lambda i, at: part.at[:, i, at], mx, x_ring, opp1.at[1, k], main1.at[1, k], self.start + count
                    ),
                ),
                (
                    RingSum(lambda i, at: q_a.at[k, i, at], mx, x_ring, opp2.at[0, k], main2.at[0, k], 0),
                    RingSum(lambda i, at: q_b.at[k, i, at], my, y_ring, opp2.at[1, k], main2.at[1, k], 0),
                ),
            )

        def arrive(self):
            lo = cap if self.k == 0 else 0
            got = x_all.at[my, mx, pl.ds(self.start + lo, 2 * count - lo)]
            pltpu.make_async_copy(got, got, z_recv.at[self.chunk]).wait()

        def compute(self):
            if self is pairs[0]:
                for name in ("eg", "eu", "ed"):
                    loads[name].wait()
            experts(self.start, 2 * count)

        def sum_start(self, phase):
            for ring in self.sums[phase]:
                ring.across(self.group, 4 + 2 * phase)
            for ring in self.sums[phase]:
                ring.plain(self.group, 5 + 2 * phase)

        def sum_relay(self, phase):
            await_rows(recv_of(self.group, 4 + 2 * phase), (8, 2)[phase], count)
            for ring in self.sums[phase]:
                ring.added(self.group, 5 + 2 * phase)

        def sum_finish(self, phase):
            await_rows(recv_of(self.group, 5 + 2 * phase), (16, 4)[phase], count)
            if phase == 0:
                targets = q_a.at[self.k], q_b.at[self.k]
            else:
                targets = y_own.at[pl.ds(self.start, count)], y_own.at[pl.ds(self.start + count, count)]
            for ring, dst in zip(self.sums[phase], targets):
                ring.total(dst)

        def send_back(self):
            if self.k == 0:
                back[0:cap, :] = y_own[0:cap, :]
            for i in range(self.k == 0, per_pair):
                at = pl.ds(pl.multiple_of(self.start + i * cap, cap), cap)
                low, high = (peer(chunk * per_pair + i) for chunk in self.chunks)
                pltpu.make_async_remote_copy(
                    src_ref=y_own.at[at], dst_ref=back.at[at], send_sem=zb_send, recv_sem=zb_recv,
                    device_id={"ep": by_half(low, high), "tp": tp}, device_id_type=MESH,
                ).start()

    pairs = [Pair(k) for k in range(n_pairs)]

    def plain_outputs():
        items[0].gather_finish(1)
        items[-1].gather_finish(1)
        for name in ("po_a", "po_b", "sd"):
            loads[name].wait()
        lane = lax.broadcasted_iota(jnp.int32, (tok // 2, LANES), 1)
        zero = jnp.zeros((tok // 2, LANES), BF16)
        upper, lower = [], []
        for i in range(n_tp):
            block = x_all[i // SIDE, i % SIDE, pool_start:pool_start + tok // 2, :]
            upper.append(jnp.where(lane < narrow, block, zero))
            lower.append(jnp.where(lane < narrow, zero, block))
        lhs = jnp.concatenate([jnp.concatenate(upper, axis=1), jnp.concatenate(lower, axis=1)], axis=0)
        out_ref[0] = dot(lhs, po2[...].reshape(2 * n_tp * narrow, LANES)).astype(BF16)
        lhs = jnp.concatenate([x_all[i // SIDE, i % SIDE, shared_rows, :] for i in range(n_tp)], axis=1)
        result = dot(lhs, sd[...])
        return result

    items = [Rows(rows_all, tok, n_pairs)] + pairs + [Rows(pool_start, tok // 2, n_pairs + 1)]

    def gathered(index):
        return items[index] if 0 <= index < len(items) else None

    def summed(index):
        return pairs[index - 1] if 1 <= index <= n_pairs else None

    for s in range(n_pairs + 1 + LAGS["close"]):
        if s == POOL_TICK:
            pool_norm(*pool_state)
        if p := gathered(s - LAGS["along"]):
            p.gather_finish(0)
            p.gather_start(1)
        if p := gathered(s - LAGS["relay"]):
            p.gather_relay(0)
        if p := gathered(s - LAGS["along_relay"]):
            p.gather_relay(1)
        if p := gathered(s):
            p.arrive()
            p.gather_start(0)
        if s == DISPATCH_TICK:
            dispatch([k for j in range(quarter) for k in (middle + j, quarter + j)] + list(range(middle + quarter, n_pairs)))
        if s == 0:
            pooled_in, halo = mix_local()
        if s == 2:
            combine_terms()
        if s == WINDOW_TICK:
            pool_state = windows(pooled_in, halo)
        if p := summed(s - LAGS["close"]):
            p.sum_finish(1)
            p.send_back()
        if p := summed(s - LAGS["second_relay"]):
            p.sum_relay(1)
        if p := summed(s - LAGS["second"]):
            p.sum_finish(0)
            p.sum_start(1)
        if p := summed(s - LAGS["first_relay"]):
            p.sum_relay(0)
        if p := summed(s - LAGS["compute"]):
            p.gather_finish(1)
            p.compute()
            p.sum_start(0)
        if s == n_pairs - 1 + LAGS["close"]:
            result = plain_outputs()

    over = (((0,), (0,)), ((), ()))
    arrived = back.at[pl.ds(cap, rows_all - cap)]
    pltpu.make_async_copy(arrived, arrived, zb_recv).wait()
    result += lax.dot_general(chi[...], back[...], over, preferred_element_type=F32)
    result += lax.dot_general(clo[...], back[...], over, preferred_element_type=F32)
    out_ref[1] = result.astype(BF16)

    halo.wait_send()
    sent = [part.at[0:2, :, 0:30 * count]] * 4 + [part.at[0, 0:2, 0:15 * p.count] for p in (items[0], items[-1])]
    for at, gone in enumerate(sent):
        pltpu.make_async_copy(gone, gone, send_sems.at[at]).wait()
    for whole, sem in ((outgoing, z_send), (y_own, zb_send)):
        gone = whole.at[pl.ds(cap, rows_all - cap)]
        pltpu.make_async_copy(gone, gone, sem).wait()
    pltpu.make_async_copy(sq_in, sq_in, sq_send.at[0]).wait()


def on_device(n_pairs, mix_input, expert_input, mix_gain, moe_gain, pool_in, pool_scale, pool_gain, pool_out, route,
              route_score, expert_gate, expert_up, expert_down, shared_gate, shared_up, shared_down):
    n_ep, n_tp = lax.axis_size("ep"), lax.axis_size("tp")
    tok, width = mix_input.shape
    top = route.shape[1]
    cap = 2 * tok * top // n_ep
    rows = cap * n_ep
    narrow = pool_in.shape[1]
    count = rows // (2 * n_pairs)
    everything = rows + tok + tok // 2
    vmem = pl.BlockSpec(memory_space=pltpu.VMEM)
    hbm = pl.BlockSpec(memory_space=pltpu.HBM)
    dma = pltpu.SemaphoreType.DMA
    both = pl.pallas_call(
        functools.partial(kernel, n_pairs),
        out_shape=jax.ShapeDtypeStruct((2, tok, shared_down.shape[1]), BF16),
        in_specs=[hbm, hbm, vmem, vmem, hbm, vmem, vmem, hbm, vmem, vmem, hbm, hbm, hbm, hbm, hbm, hbm],
        out_specs=vmem,
        scratch_shapes=[
            pltpu.VMEM((tok, width), BF16),
            pltpu.VMEM((tok, width), BF16),
            pltpu.VMEM((width, 2 * LANES), BF16),
            pltpu.VMEM((LANES, width), BF16),
            pltpu.VMEM((width, 2 * LANES), BF16),
            pltpu.VMEM((width, LANES), BF16),
            pltpu.VMEM((narrow, width), BF16),
            pltpu.VMEM((n_tp, 2, narrow, LANES), BF16),
            pltpu.VMEM((tok, width), BF16),
            pltpu.VMEM((tok, width), BF16),
            pltpu.VMEM((rows, LANES), BF16),
            pltpu.VMEM((rows, LANES), BF16),
            pltpu.VMEM((rows, LANES), BF16),
            pltpu.VMEM((rows, LANES), BF16),
            pltpu.VMEM((SIDE, SIDE, everything, LANES), BF16),
            pltpu.VMEM((SIDE, SIDE, rows, LANES), BF16),
            pltpu.VMEM((n_pairs, SIDE, count, LANES), BF16),
            pltpu.VMEM((n_pairs, SIDE, count, LANES), BF16),
            pltpu.VMEM((rows, LANES), BF16),
            pltpu.VMEM((rows, LANES), BF16),
            pltpu.VMEM((2, n_pairs, 2, SIDE, count // 2, LANES), BF16),
            pltpu.VMEM((2, n_pairs, 2, SIDE, count, LANES), BF16),
            pltpu.VMEM((2, n_pairs, 2, count // 2, LANES), BF16),
            pltpu.VMEM((2, n_pairs, 2, count, LANES), BF16),
            pltpu.VMEM((16, LANES), BF16),
            pltpu.VMEM((16, LANES), BF16),
            pltpu.VMEM((8, LANES), F32),
            pltpu.VMEM((n_tp - 1, 8, LANES), F32),
            dma((11,)),
            dma((6,)),
            dma((n_pairs, 8)),
            dma((2, 4)),
            dma,
            dma((n_pairs,)),
            dma,
            dma,
            dma((2,)),
            dma((2,)),
        ],
        compiler_params=pltpu.CompilerParams(
            collective_id=0, has_side_effects=True, vmem_limit_bytes=60 * 1024 * 1024
        ),
    )(
        expert_input,
        mix_input,
        mix_gain.reshape(1, -1),
        moe_gain.reshape(1, -1),
        pool_in.T,
        pool_scale.reshape(1, -1),
        pool_gain.reshape(1, -1),
        pool_out.reshape(n_tp, narrow, pool_out.shape[1]),
        route.T,
        route_score.T,
        expert_gate,
        expert_up,
        expert_down,
        shared_gate,
        shared_up,
        shared_down,
    )
    return both[0], both[1]


def solution(mesh):
    return jax.shard_map(
        functools.partial(on_device, 16),
        mesh=mesh,
        in_specs=(
            P("ep", None),
            P("ep", None),
            P(),
            P(),
            P(None, "tp"),
            P("tp"),
            P("tp"),
            P(None, "tp"),
            P("ep", None),
            P("ep", None),
            P("ep", None, "tp"),
            P("ep", None, "tp"),
            P("ep", "tp", None),
            P(None, "tp"),
            P(None, "tp"),
            P(None, "tp"),
        ),
        out_specs=(P("ep", "tp"), P("ep", "tp")),
        check_vma=False,
    )
```

```python
import functools

import jax
import jax.numpy as jnp
from jax import lax
from jax.experimental import pallas as pl
from jax.experimental.pallas import tpu as pltpu
from jax.sharding import PartitionSpec as P

MESH = pl.DeviceIdType.MESH
F32, BF16 = jnp.float32, jnp.bfloat16
EPS = 1e-06
SIDE = 4
DISPATCH_TICKS, WINDOW_TICK, POOL_TICK = (1, 3, 6), 8, 14
LAGS = {"relay": 2, "along": 4, "along_relay": 6, "compute": 8, "first_relay": 10, "second": 12, "second_relay": 14, "close": 16}
LANES = 128


def dot(a, b):
    return jnp.dot(a, b, preferred_element_type=F32)


def silu_mul(gate, upper):
    return gate / (1.0 + jnp.exp(-gate)) * upper


def kernel(
    n_pairs,
    xe_hbm, xm_hbm, mix_gain_ref, moe_gain_ref, pin_hbm, pscale_ref, pgain_ref, pout_hbm, route_ref, score_ref,
    eg_hbm, eu_hbm, ed_hbm, sg_hbm, su_hbm, sd_hbm,
    out_ref,
    xe, xm, wgu, wd, sgu, sd, pin, po2, mn, mm, sel, chi, clo, outgoing, x_all, part, q_a, q_b, y_own, back,
    opp1, main1, opp2, main2, halo_out, halo_in, sq_out, sq_in,
    load_sems, send_sems, recv_sems, rows_sems, z_send, z_recv, zb_send, zb_recv, sq_send, sq_recv,
):
    n_ep, n_tp = lax.axis_size("ep"), lax.axis_size("tp")
    ep, tp = lax.axis_index("ep"), lax.axis_index("tp")
    n_z = n_ep // 2
    z, core = ep // 2, ep % 2
    my, mx = tp // SIDE, tp % SIDE
    tok, width = xe_hbm.shape
    rows_all = outgoing.shape[0]
    cap = rows_all // n_ep

    def wrap(value, size):
        return lax.rem(value, size)

    z_bits = [wrap(z // 2 ** b, 2) for b in range(8) if 2 ** b < n_z]
    late = z // (n_z // 2)

    def peer(i):
        other = z
        for b, bit in enumerate(z_bits):
            if i // 2 // 2 ** b % 2:
                other = other + 2 ** b * (1 - 2 * bit)
        return other * 2 + wrap(core + i % 2, 2)

    def by_half(low, high):
        return low if isinstance(low, int) and low == high else low + late * (high - low)

    loads = {}

    def load(name, src, dst):
        loads[name] = pltpu.make_async_copy(src, dst, load_sems.at[len(loads)])
        loads[name].start()

    load("xe", xe_hbm, xe)

    barrier = pltpu.get_barrier_semaphore()
    for i in range(n_ep - 1, 0, -1):
        pl.semaphore_signal(barrier, inc=1, device_id={"ep": peer(i), "tp": tp}, device_id_type=MESH)
    for i in range(1, n_tp):
        pl.semaphore_signal(barrier, inc=1, device_id={"ep": ep, "tp": wrap(tp + i, n_tp)}, device_id_type=MESH)

    load("xm", xm_hbm, xm)
    load("pin", pin_hbm, pin)
    load("sg", sg_hbm, sgu.at[:, 0:LANES])
    load("su", su_hbm, sgu.at[:, LANES:2 * LANES])
    load("eg", eg_hbm.at[0], wgu.at[:, 0:LANES])
    load("eu", eu_hbm.at[0], wgu.at[:, LANES:2 * LANES])
    load("ed", ed_hbm.at[0], wd)
    load("po_a", pout_hbm, po2.at[:, 0])
    load("po_b", pout_hbm, po2.at[:, 1])
    load("sd", sd_hbm, sd)

    def row_norm(src, gain_ref, dst):
        for b in range(tok // 16):
            at = slice(b * 16, (b + 1) * 16)
            values = src[at, :].astype(F32)
            scale = lax.rsqrt(jnp.mean(values * values, axis=-1, keepdims=True) + EPS)
            dst[at, :] = (values * scale * gain_ref[...]).astype(BF16)


    top = route_ref.shape[0]
    routes = [route_ref[k:k + 1, :].astype(F32) for k in range(top)]
    scores = [score_ref[k:k + 1, :] for k in range(top)]
    slot_i = lax.broadcasted_iota(jnp.int32, (n_ep, tok), 0)
    expert_i = (((slot_i // 2) ^ z) * 2 + ((slot_i % 2) ^ core)).astype(F32)
    total = scores[0]
    for k in range(1, top):
        total = total + scores[k]
    hit = jnp.zeros((n_ep, tok), F32)
    weight = jnp.zeros((n_ep, tok), F32)
    for k in range(top):
        same = expert_i == routes[k]
        hit = jnp.where(same, 1.0, hit)
        weight = jnp.where(same, 2.5 * scores[k] / total, weight)
    before = (
        lax.broadcasted_iota(jnp.int32, (tok, tok), 0) < lax.broadcasted_iota(jnp.int32, (tok, tok), 1)
    )
    rank = dot(hit.astype(BF16), jnp.where(before, 1.0, 0.0).astype(BF16))
    place = jnp.where(hit > 0.0, rank, -1.0)
    slot_row = lax.broadcasted_iota(jnp.int32, (cap, tok), 0).astype(F32)
    for i in range(n_ep):
        sel[i * cap:(i + 1) * cap, :] = jnp.where(place[i:i + 1, :] == slot_row, 1.0, 0.0).astype(BF16)

    loads["xe"].wait()
    row_norm(xe, moe_gain_ref, mn)
    share = mn[:, pl.ds(pl.multiple_of(tp * LANES, LANES), LANES)]
    outgoing[...] = dot(sel[...], share).astype(BF16)
    x_all[my, mx, 0:cap, :] = outgoing[0:cap, :]

    loads["sg"].wait()
    loads["su"].wait()
    both = dot(mn[...], sgu[...])
    shared_rows = slice(rows_all, rows_all + tok)
    x_all[my, mx, shared_rows, :] = silu_mul(both[:, :LANES], both[:, LANES:]).astype(BF16)

    pl.semaphore_wait(barrier, n_ep - 1 + n_tp - 1)

    middle, quarter = n_pairs // 2, n_pairs // 4
    low_order = list(range(n_pairs - 2)) + [n_pairs - 1, n_pairs - 2]
    third, fourth = list(range(middle, middle + quarter)), list(range(middle + quarter, n_pairs))
    high_order = list(range(quarter)) + fourth + third + list(range(middle - 1, quarter - 1, -1))
    per_pair = n_ep // n_pairs

    def dispatch(chunks):
        for i in [i for k in chunks for i in range(max(1, k * per_pair), (k + 1) * per_pair)]:
            at = pl.ds(i * cap, cap)
            pltpu.make_async_remote_copy(
                src_ref=outgoing.at[at], dst_ref=x_all.at[my, mx, at], send_sem=z_send,
                recv_sem=z_recv.at[i // per_pair], device_id={"ep": peer(i), "tp": tp}, device_id_type=MESH,
            ).start()

    dispatch(range(quarter))

    def dispatch_later(turn):
        second = list(range(quarter, middle))
        low = ([k for pair in zip(fourth, second) for k in pair], third, [])[turn]
        high = ([], third + fourth, second[::-1])[turn]

        @pl.when(late == 0)
        def _():
            dispatch(low)

        @pl.when(late == 1)
        def _():
            dispatch(high)

    x_ring = lambda step: {"ep": ep, "tp": my * SIDE + wrap(mx + step, SIDE)}
    y_ring = lambda step: {"ep": ep, "tp": wrap(my + step, SIDE) * SIDE + mx}

    def send_of(group):
        return send_sems.at[group // quarter if group < n_pairs else 4 + group - n_pairs]

    def recv_of(group, stage):
        return recv_sems.at[group, stage] if group < n_pairs else rows_sems.at[group - n_pairs, stage]

    def launch(group, stage, src, dst, where):
        pltpu.make_async_remote_copy(
            src_ref=src, dst_ref=dst, send_sem=send_of(group), recv_sem=recv_of(group, stage),
            device_id=where, device_id_type=MESH,
        ).start()

    def await_rows(sem, units, rows):
        spot = {2: part.at[0, 0:2, 0:rows], 4: part.at[0, :, 0:rows], 8: part.at[0:2, :, 0:rows],
                16: part.at[:, :, 0:rows]}[units]
        pltpu.make_async_copy(spot, spot, sem).wait()

    class Ring:
        def __init__(self, view, me, ring, start, count):
            self.view, self.me, self.ring, self.start_row, self.count = view, me, ring, start, count

        def unit(self, step, half=None):
            lo, n = (0, self.count) if half is None else (half * self.count // 2, self.count // 2)
            return self.view(wrap(self.me + step, SIDE), pl.ds(self.start_row + lo, n))

        def own(self, group, stage):
            unit = self.unit(0)
            launch(group, stage, unit, unit, self.ring(1))
            launch(group, stage, unit, unit, self.ring(SIDE - 1))

        def onward(self, group, stage):
            first, second = self.unit(SIDE - 1, 0), self.unit(1, 1)
            launch(group, stage, first, first, self.ring(1))
            launch(group, stage, second, second, self.ring(SIDE - 1))

    class Rows:
        def __init__(self, start, rows, group):
            self.group, self.count = group, rows // 2
            a, b = (start, self.count), (start + self.count, self.count)
            self.rings = (
                (
                    Ring(lambda i, at: x_all.at[my, i, at], mx, x_ring, *a),
                    Ring(lambda i, at: x_all.at[i, mx, at], my, y_ring, *b),
                ),
                (
                    Ring(lambda i, at: x_all.at[i, :, at], my, y_ring, *a),
                    Ring(lambda i, at: x_all.at[:, i, at], mx, x_ring, *b),
                ),
            )

        def arrive(self):
            pass

        def gather_start(self, phase):
            for ring in self.rings[phase]:
                ring.own(self.group, 2 * phase)

        def gather_relay(self, phase):
            await_rows(recv_of(self.group, 2 * phase), (4, 16)[phase], self.count)
            for ring in self.rings[phase]:
                ring.onward(self.group, 2 * phase + 1)

        def gather_finish(self, phase):
            await_rows(recv_of(self.group, 2 * phase + 1), (2, 8)[phase], self.count)

    narrow = pin.shape[0]

    def mix_local():
        loads["xm"].wait()
        row_norm(xm, mix_gain_ref, mm)
        loads["pin"].wait()
        pooled_in = lax.dot_general(mm[...], pin[...], (((1,), (1,)), ((), ())), preferred_element_type=F32)
        pooled_in = jnp.concatenate([pooled_in, jnp.zeros((tok, LANES - narrow), F32)], axis=1).astype(BF16)
        halo_out[...] = pooled_in[tok - 16:, :]
        halo = pltpu.make_async_remote_copy(
            src_ref=halo_out, dst_ref=halo_in, send_sem=sq_send.at[1], recv_sem=sq_recv.at[1],
            device_id={"ep": wrap(ep + 1, n_ep), "tp": tp}, device_id_type=MESH,
        )
        halo.start()
        return pooled_in, halo

    def windows(pooled_in, halo):
        halo.wait_recv()
        carried = jnp.where(ep > 0, halo_in[...].astype(F32), 0.0)
        ext = jnp.concatenate([carried, pooled_in.astype(F32)], axis=0)
        sums, chosen, window = ext, None, 1
        for index in range(4):
            sums = sums + pltpu.roll(sums, window, 0)
            window *= 2
            chosen = sums if chosen is None else jnp.where(my >= index, sums, chosen)
        position = (ep * tok + lax.broadcasted_iota(jnp.int32, (tok, LANES), 0) + 1).astype(F32)
        widest = lax.shift_left(2, my).astype(F32)
        zeros_right = jnp.zeros((1, LANES - narrow), F32)
        pscale = jnp.concatenate([pscale_ref[...], zeros_right], axis=1)
        pgain = jnp.concatenate([pgain_ref[...], zeros_right], axis=1)
        scaled = (chosen[16:, :] / jnp.minimum(position, widest) - pooled_in.astype(F32)) * pscale
        squares = jnp.sum(scaled * scaled, axis=1, keepdims=True)
        squares = jnp.broadcast_to(squares, (tok, LANES)).T[0:8, :]
        sq_out[...] = squares

        for i in range(1, n_tp):
            pltpu.make_async_remote_copy(
                src_ref=sq_out, dst_ref=sq_in.at[i - 1], send_sem=sq_send.at[0], recv_sem=sq_recv.at[0],
                device_id={"ep": ep, "tp": wrap(tp + i, n_tp)}, device_id_type=MESH,
            ).start()
        return scaled, squares, pgain

    def combine_terms():
        high = weight.astype(BF16).astype(F32)
        low = weight - high
        for i in range(n_ep):
            at = slice(i * cap, (i + 1) * cap)
            same = place[i:i + 1, :] == slot_row
            chi[at, :] = jnp.where(same, high[i:i + 1, :], 0.0).astype(BF16)
            clo[at, :] = jnp.where(same, low[i:i + 1, :], 0.0).astype(BF16)

    pool_start = rows_all + tok

    def pool_norm(scaled, squares, pgain):
        pltpu.make_async_copy(sq_in, sq_in, sq_recv.at[0]).wait()
        total = squares
        for i in range(n_tp - 1):
            total = total + sq_in[i]
        total = jnp.broadcast_to(total[0:1, :], (tok, LANES)).T
        pooled = (scaled * lax.rsqrt(total / (narrow * n_tp) + EPS) * pgain).astype(BF16).astype(F32)
        packed = pooled[:tok // 2, :] + pltpu.roll(pooled[tok // 2:, :], narrow, 1)
        x_all[my, mx, pool_start:pool_start + tok // 2, :] = packed.astype(BF16)

    count = rows_all // (2 * n_pairs)
    half = count // 2

    class RingSum:
        def __init__(self, view, me, ring, opp, main, start):
            self.view, self.me, self.ring, self.opp, self.main, self.start_row = view, me, ring, opp, main, start

        def unit(self, step, which=None):
            lo, n = (0, count) if which is None else (which * half, half)
            return self.view(wrap(self.me + step, SIDE), pl.ds(self.start_row + lo, n))

        def into(self, side, which):
            at = pl.ds(which * half, half)
            return self.main.at[(side,) + (slice(None),) * (len(self.main.shape) - 3) + (at,)]

        def across(self, group, stage):
            launch(group, stage, self.unit(2, 0), self.opp.at[0], self.ring(1))
            launch(group, stage, self.unit(2, 1), self.opp.at[1], self.ring(SIDE - 1))

        def plain(self, group, stage):
            launch(group, stage, self.unit(1, 1), self.into(0, 1), self.ring(1))
            launch(group, stage, self.unit(SIDE - 1, 0), self.into(1, 0), self.ring(SIDE - 1))

        def added(self, group, stage):
            for unit, extra, dst, where in (
                (self.unit(1, 0), self.opp.at[0], self.into(0, 0), self.ring(1)),
                (self.unit(SIDE - 1, 1), self.opp.at[1], self.into(1, 1), self.ring(SIDE - 1)),
            ):
                unit[...] = (unit[...].astype(F32) + extra[...].astype(F32)).astype(BF16)
                launch(group, stage, unit, dst, where)

        def total(self, dst):
            own = self.unit(0)
            dst[...] = (own[...].astype(F32) + self.main[0].astype(F32) + self.main[1].astype(F32)).astype(BF16)

    tile = min(256, 2 * count)

    def experts(start, rows):
        @pl.loop(0, rows // tile)
        def _(b):
            at = pl.ds(pl.multiple_of(start + b * tile, tile), tile)
            lhs = jnp.concatenate([x_all[i // SIDE, i % SIDE, at, :] for i in range(n_tp)], axis=1)
            pair = dot(lhs, wgu[...])
            hidden = silu_mul(pair[:, :LANES], pair[:, LANES:]).astype(BF16)
            for j in range(n_tp // 2):
                out = dot(hidden, wd[:, j * 2 * LANES:(j + 1) * 2 * LANES])
                for s in range(2):
                    i = 2 * j + s
                    part[i // SIDE, i % SIDE, at, :] = out[:, s * LANES:(s + 1) * LANES].astype(BF16)

    class Pair(Rows):
        def __init__(self, k):
            self.k, self.chunks = k, (low_order[k], high_order[k])
            self.chunk = by_half(*self.chunks)
            self.start = self.chunk * (2 * count)
            if k > 0:
                self.start = pl.multiple_of(self.start, 2 * count)
            super().__init__(self.start, 2 * count, k)
            self.sums = (
                (
                    RingSum(lambda i, at: part.at[i, :, at], my, y_ring, opp1.at[0, k], main1.at[0, k], self.start),
                    RingSum(
                        lambda i, at: part.at[:, i, at], mx, x_ring, opp1.at[1, k], main1.at[1, k], self.start + count
                    ),
                ),
                (
                    RingSum(lambda i, at: q_a.at[k, i, at], mx, x_ring, opp2.at[0, k], main2.at[0, k], 0),
                    RingSum(lambda i, at: q_b.at[k, i, at], my, y_ring, opp2.at[1, k], main2.at[1, k], 0),
                ),
            )

        def arrive(self):
            lo = cap if self.k == 0 else 0
            got = x_all.at[my, mx, pl.ds(self.start + lo, 2 * count - lo)]
            pltpu.make_async_copy(got, got, z_recv.at[self.chunk]).wait()

        def compute(self):
            if self is pairs[0]:
                for name in ("eg", "eu", "ed"):
                    loads[name].wait()
            experts(self.start, 2 * count)

        def sum_start(self, phase):
            for ring in self.sums[phase]:
                ring.across(self.group, 4 + 2 * phase)
            for ring in self.sums[phase]:
                ring.plain(self.group, 5 + 2 * phase)

        def sum_relay(self, phase):
            await_rows(recv_of(self.group, 4 + 2 * phase), (8, 2)[phase], count)
            for ring in self.sums[phase]:
                ring.added(self.group, 5 + 2 * phase)

        def sum_finish(self, phase):
            await_rows(recv_of(self.group, 5 + 2 * phase), (16, 4)[phase], count)
            if phase == 0:
                targets = q_a.at[self.k], q_b.at[self.k]
            else:
                targets = y_own.at[pl.ds(self.start, count)], y_own.at[pl.ds(self.start + count, count)]
            for ring, dst in zip(self.sums[phase], targets):
                ring.total(dst)

        def send_back(self):
            if self.k == 0:
                back[0:cap, :] = y_own[0:cap, :]
            for i in range(self.k == 0, per_pair):
                at = pl.ds(pl.multiple_of(self.start + i * cap, cap), cap)
                low, high = (peer(chunk * per_pair + i) for chunk in self.chunks)
                pltpu.make_async_remote_copy(
                    src_ref=y_own.at[at], dst_ref=back.at[at], send_sem=zb_send, recv_sem=zb_recv,
                    device_id={"ep": by_half(low, high), "tp": tp}, device_id_type=MESH,
                ).start()

    pairs = [Pair(k) for k in range(n_pairs)]

    def plain_outputs():
        items[0].gather_finish(1)
        items[-1].gather_finish(1)
        for name in ("po_a", "po_b", "sd"):
            loads[name].wait()
        lane = lax.broadcasted_iota(jnp.int32, (tok // 2, LANES), 1)
        zero = jnp.zeros((tok // 2, LANES), BF16)
        upper, lower = [], []
        for i in range(n_tp):
            block = x_all[i // SIDE, i % SIDE, pool_start:pool_start + tok // 2, :]
            upper.append(jnp.where(lane < narrow, block, zero))
            lower.append(jnp.where(lane < narrow, zero, block))
        lhs = jnp.concatenate([jnp.concatenate(upper, axis=1), jnp.concatenate(lower, axis=1)], axis=0)
        out_ref[0] = dot(lhs, po2[...].reshape(2 * n_tp * narrow, LANES)).astype(BF16)
        lhs = jnp.concatenate([x_all[i // SIDE, i % SIDE, shared_rows, :] for i in range(n_tp)], axis=1)
        result = dot(lhs, sd[...])
        return result

    items = [Rows(rows_all, tok, n_pairs)] + pairs + [Rows(pool_start, tok // 2, n_pairs + 1)]

    def gathered(index):
        return items[index] if 0 <= index < len(items) else None

    def summed(index):
        return pairs[index - 1] if 1 <= index <= n_pairs else None

    for s in range(n_pairs + 1 + LAGS["close"]):
        if s == POOL_TICK:
            pool_norm(*pool_state)
        if p := gathered(s - LAGS["along"]):
            p.gather_finish(0)
            p.gather_start(1)
        if p := gathered(s - LAGS["relay"]):
            p.gather_relay(0)
        if p := gathered(s - LAGS["along_relay"]):
            p.gather_relay(1)
        if p := gathered(s):
            p.arrive()
            p.gather_start(0)
        if s in DISPATCH_TICKS:
            dispatch_later(DISPATCH_TICKS.index(s))
        if s == 0:
            pooled_in, halo = mix_local()
        if s == 2:
            combine_terms()
        if s == WINDOW_TICK:
            pool_state = windows(pooled_in, halo)
        if p := summed(s - LAGS["close"]):
            p.sum_finish(1)
            p.send_back()
        if p := summed(s - LAGS["second_relay"]):
            p.sum_relay(1)
        if p := summed(s - LAGS["second"]):
            p.sum_finish(0)
            p.sum_start(1)
        if p := summed(s - LAGS["first_relay"]):
            p.sum_relay(0)
        if p := summed(s - LAGS["compute"]):
            p.gather_finish(1)
            p.compute()
            p.sum_start(0)
        if s == n_pairs - 1 + LAGS["close"]:
            result = plain_outputs()

    over = (((0,), (0,)), ((), ()))
    arrived = back.at[pl.ds(cap, rows_all - cap)]
    pltpu.make_async_copy(arrived, arrived, zb_recv).wait()
    result += lax.dot_general(chi[...], back[...], over, preferred_element_type=F32)
    result += lax.dot_general(clo[...], back[...], over, preferred_element_type=F32)
    out_ref[1] = result.astype(BF16)

    halo.wait_send()
    sent = [part.at[0:2, :, 0:30 * count]] * 4 + [part.at[0, 0:2, 0:15 * p.count] for p in (items[0], items[-1])]
    for at, gone in enumerate(sent):
        pltpu.make_async_copy(gone, gone, send_sems.at[at]).wait()
    for whole, sem in ((outgoing, z_send), (y_own, zb_send)):
        gone = whole.at[pl.ds(cap, rows_all - cap)]
        pltpu.make_async_copy(gone, gone, sem).wait()
    pltpu.make_async_copy(sq_in, sq_in, sq_send.at[0]).wait()


def on_device(n_pairs, mix_input, expert_input, mix_gain, moe_gain, pool_in, pool_scale, pool_gain, pool_out, route,
              route_score, expert_gate, expert_up, expert_down, shared_gate, shared_up, shared_down):
    n_ep, n_tp = lax.axis_size("ep"), lax.axis_size("tp")
    tok, width = mix_input.shape
    top = route.shape[1]
    cap = 2 * tok * top // n_ep
    rows = cap * n_ep
    narrow = pool_in.shape[1]
    count = rows // (2 * n_pairs)
    everything = rows + tok + tok // 2
    vmem = pl.BlockSpec(memory_space=pltpu.VMEM)
    hbm = pl.BlockSpec(memory_space=pltpu.HBM)
    dma = pltpu.SemaphoreType.DMA
    both = pl.pallas_call(
        functools.partial(kernel, n_pairs),
        out_shape=jax.ShapeDtypeStruct((2, tok, shared_down.shape[1]), BF16),
        in_specs=[hbm, hbm, vmem, vmem, hbm, vmem, vmem, hbm, vmem, vmem, hbm, hbm, hbm, hbm, hbm, hbm],
        out_specs=vmem,
        scratch_shapes=[
            pltpu.VMEM((tok, width), BF16),
            pltpu.VMEM((tok, width), BF16),
            pltpu.VMEM((width, 2 * LANES), BF16),
            pltpu.VMEM((LANES, width), BF16),
            pltpu.VMEM((width, 2 * LANES), BF16),
            pltpu.VMEM((width, LANES), BF16),
            pltpu.VMEM((narrow, width), BF16),
            pltpu.VMEM((n_tp, 2, narrow, LANES), BF16),
            pltpu.VMEM((tok, width), BF16),
            pltpu.VMEM((tok, width), BF16),
            pltpu.VMEM((rows, LANES), BF16),
            pltpu.VMEM((rows, LANES), BF16),
            pltpu.VMEM((rows, LANES), BF16),
            pltpu.VMEM((rows, LANES), BF16),
            pltpu.VMEM((SIDE, SIDE, everything, LANES), BF16),
            pltpu.VMEM((SIDE, SIDE, rows, LANES), BF16),
            pltpu.VMEM((n_pairs, SIDE, count, LANES), BF16),
            pltpu.VMEM((n_pairs, SIDE, count, LANES), BF16),
            pltpu.VMEM((rows, LANES), BF16),
            pltpu.VMEM((rows, LANES), BF16),
            pltpu.VMEM((2, n_pairs, 2, SIDE, count // 2, LANES), BF16),
            pltpu.VMEM((2, n_pairs, 2, SIDE, count, LANES), BF16),
            pltpu.VMEM((2, n_pairs, 2, count // 2, LANES), BF16),
            pltpu.VMEM((2, n_pairs, 2, count, LANES), BF16),
            pltpu.VMEM((16, LANES), BF16),
            pltpu.VMEM((16, LANES), BF16),
            pltpu.VMEM((8, LANES), F32),
            pltpu.VMEM((n_tp - 1, 8, LANES), F32),
            dma((11,)),
            dma((6,)),
            dma((n_pairs, 8)),
            dma((2, 4)),
            dma,
            dma((n_pairs,)),
            dma,
            dma,
            dma((2,)),
            dma((2,)),
        ],
        compiler_params=pltpu.CompilerParams(
            collective_id=0, has_side_effects=True, vmem_limit_bytes=60 * 1024 * 1024
        ),
    )(
        expert_input,
        mix_input,
        mix_gain.reshape(1, -1),
        moe_gain.reshape(1, -1),
        pool_in.T,
        pool_scale.reshape(1, -1),
        pool_gain.reshape(1, -1),
        pool_out.reshape(n_tp, narrow, pool_out.shape[1]),
        route.T,
        route_score.T,
        expert_gate,
        expert_up,
        expert_down,
        shared_gate,
        shared_up,
        shared_down,
    )
    return both[0], both[1]


def solution(mesh):
    return jax.shard_map(
        functools.partial(on_device, 16),
        mesh=mesh,
        in_specs=(
            P("ep", None),
            P("ep", None),
            P(),
            P(),
            P(None, "tp"),
            P("tp"),
            P("tp"),
            P(None, "tp"),
            P("ep", None),
            P("ep", None),
            P("ep", None, "tp"),
            P("ep", None, "tp"),
            P("ep", "tp", None),
            P(None, "tp"),
            P(None, "tp"),
            P(None, "tp"),
        ),
        out_specs=(P("ep", "tp"), P("ep", "tp")),
        check_vma=False,
    )
```

```python
import functools

import jax
import jax.numpy as jnp
from jax import lax
from jax.experimental import pallas as pl
from jax.experimental.pallas import tpu as pltpu
from jax.sharding import PartitionSpec as P

MESH = pl.DeviceIdType.MESH
F32, BF16 = jnp.float32, jnp.bfloat16
EPS = 1e-06
SIDE = 4
DISPATCH_TICKS, WINDOW_TICK, POOL_TICK = (1, 3, 6), 8, 14
LAGS = {"relay": 2, "along": 4, "along_relay": 6, "compute": 8, "first_relay": 10, "second": 12, "second_relay": 14, "close": 16}
LANES = 128


def dot(a, b):
    return jnp.dot(a, b, preferred_element_type=F32)


def silu_mul(gate, upper):
    return gate / (1.0 + jnp.exp(-gate)) * upper


def kernel(
    n_pairs,
    xe_hbm, xm_hbm, mix_gain_ref, moe_gain_ref, pin_hbm, pscale_ref, pgain_ref, pout_hbm, route_ref, score_ref,
    eg_hbm, eu_hbm, ed_hbm, sg_hbm, su_hbm, sd_hbm,
    out_ref,
    xe, xm, wgu, wd, sgu, sd, pin, po2, mn, mm, sel, chi, clo, outgoing, x_all, part, q_a, q_b, y_own, back,
    opp1, main1, opp2, main2, halo_out, halo_in, sq_out, sq_in,
    load_sems, send_sems, recv_sems, rows_sems, z_send, z_recv, zb_send, zb_recv, sq_send, sq_recv,
):
    n_ep, n_tp = lax.axis_size("ep"), lax.axis_size("tp")
    ep, tp = lax.axis_index("ep"), lax.axis_index("tp")
    n_z = n_ep // 2
    z, core = ep // 2, ep % 2
    my, mx = tp // SIDE, tp % SIDE
    tok, width = xe_hbm.shape
    rows_all = outgoing.shape[0]
    cap = rows_all // n_ep

    def wrap(value, size):
        return lax.rem(value, size)

    z_bits = [wrap(z // 2 ** b, 2) for b in range(8) if 2 ** b < n_z]
    late = z // (n_z // 2)

    def peer(i):
        other = z
        for b, bit in enumerate(z_bits):
            if i // 2 // 2 ** b % 2:
                other = other + 2 ** b * (1 - 2 * bit)
        return other * 2 + wrap(core + i % 2, 2)

    def by_half(low, high):
        return low if isinstance(low, int) and low == high else low + late * (high - low)

    loads = {}

    def load(name, src, dst):
        loads[name] = pltpu.make_async_copy(src, dst, load_sems.at[len(loads)])
        loads[name].start()

    load("xe", xe_hbm, xe)

    barrier = pltpu.get_barrier_semaphore()
    for i in range(n_ep - 1, 0, -1):
        pl.semaphore_signal(barrier, inc=1, device_id={"ep": peer(i), "tp": tp}, device_id_type=MESH)
    for i in range(1, n_tp):
        pl.semaphore_signal(barrier, inc=1, device_id={"ep": ep, "tp": wrap(tp + i, n_tp)}, device_id_type=MESH)

    load("xm", xm_hbm, xm)
    load("pin", pin_hbm, pin)
    load("sg", sg_hbm, sgu.at[:, 0:LANES])
    load("su", su_hbm, sgu.at[:, LANES:2 * LANES])
    load("eg", eg_hbm.at[0], wgu.at[:, 0:LANES])
    load("eu", eu_hbm.at[0], wgu.at[:, LANES:2 * LANES])
    load("ed", ed_hbm.at[0], wd)
    load("po_a", pout_hbm, po2.at[:, 0])
    load("po_b", pout_hbm, po2.at[:, 1])
    load("sd", sd_hbm, sd)

    def row_norm(src, gain_ref, dst):
        for b in range(tok // 16):
            at = slice(b * 16, (b + 1) * 16)
            values = src[at, :].astype(F32)
            scale = lax.rsqrt(jnp.mean(values * values, axis=-1, keepdims=True) + EPS)
            dst[at, :] = (values * scale * gain_ref[...]).astype(BF16)


    top = route_ref.shape[0]
    routes = [route_ref[k:k + 1, :].astype(F32) for k in range(top)]
    scores = [score_ref[k:k + 1, :] for k in range(top)]
    slot_i = lax.broadcasted_iota(jnp.int32, (n_ep, tok), 0)
    expert_i = (((slot_i // 2) ^ z) * 2 + ((slot_i % 2) ^ core)).astype(F32)
    total = scores[0]
    for k in range(1, top):
        total = total + scores[k]
    hit = jnp.zeros((n_ep, tok), F32)
    weight = jnp.zeros((n_ep, tok), F32)
    for k in range(top):
        same = expert_i == routes[k]
        hit = jnp.where(same, 1.0, hit)
        weight = jnp.where(same, 2.5 * scores[k] / total, weight)
    before = (
        lax.broadcasted_iota(jnp.int32, (tok, tok), 0) < lax.broadcasted_iota(jnp.int32, (tok, tok), 1)
    )
    rank = dot(hit.astype(BF16), jnp.where(before, 1.0, 0.0).astype(BF16))
    place = jnp.where(hit > 0.0, rank, -1.0)
    slot_row = lax.broadcasted_iota(jnp.int32, (cap, tok), 0).astype(F32)
    for i in range(n_ep):
        sel[i * cap:(i + 1) * cap, :] = jnp.where(place[i:i + 1, :] == slot_row, 1.0, 0.0).astype(BF16)

    loads["xe"].wait()
    row_norm(xe, moe_gain_ref, mn)
    share = mn[:, pl.ds(pl.multiple_of(tp * LANES, LANES), LANES)]
    outgoing[...] = dot(sel[...], share).astype(BF16)
    x_all[my, mx, 0:cap, :] = outgoing[0:cap, :]

    loads["sg"].wait()
    loads["su"].wait()
    both = dot(mn[...], sgu[...])
    shared_rows = slice(rows_all, rows_all + tok)
    x_all[my, mx, shared_rows, :] = silu_mul(both[:, :LANES], both[:, LANES:]).astype(BF16)

    pl.semaphore_wait(barrier, n_ep - 1 + n_tp - 1)

    middle, quarter = n_pairs // 2, n_pairs // 4
    low_order = list(range(n_pairs - 2)) + [n_pairs - 1, n_pairs - 2]
    third, fourth = list(range(middle, middle + quarter)), list(range(middle + quarter, n_pairs))
    high_order = list(range(quarter)) + fourth + third + list(range(middle - 1, quarter - 1, -1))
    per_pair = n_ep // n_pairs

    def dispatch(chunks):
        for i in [i for k in chunks for i in range(max(1, k * per_pair), (k + 1) * per_pair)]:
            at = pl.ds(i * cap, cap)
            pltpu.make_async_remote_copy(
                src_ref=outgoing.at[at], dst_ref=x_all.at[my, mx, at], send_sem=z_send,
                recv_sem=z_recv.at[i // per_pair], device_id={"ep": peer(i), "tp": tp}, device_id_type=MESH,
            ).start()

    dispatch(range(quarter))

    def dispatch_later(turn):
        second = list(range(quarter, middle))
        low = ([k for pair in zip(fourth, second) for k in pair], third, [])[turn]
        high = ([], third + fourth, second[::-1])[turn]

        @pl.when(late == 0)
        def _():
            dispatch(low)

        @pl.when(late == 1)
        def _():
            dispatch(high)

    x_ring = lambda step: {"ep": ep, "tp": my * SIDE + wrap(mx + step, SIDE)}
    y_ring = lambda step: {"ep": ep, "tp": wrap(my + step, SIDE) * SIDE + mx}

    def send_of(group):
        return send_sems.at[group // quarter if group < n_pairs else 4 + group - n_pairs]

    def recv_of(group, stage):
        return recv_sems.at[group % middle, stage] if group < n_pairs else rows_sems.at[group - n_pairs, stage]

    def launch(group, stage, src, dst, where):
        pltpu.make_async_remote_copy(
            src_ref=src, dst_ref=dst, send_sem=send_of(group), recv_sem=recv_of(group, stage),
            device_id=where, device_id_type=MESH,
        ).start()

    def await_rows(sem, units, rows):
        spot = {2: part.at[0, 0:2, 0:rows], 4: part.at[0, :, 0:rows], 8: part.at[0:2, :, 0:rows],
                16: part.at[:, :, 0:rows]}[units]
        pltpu.make_async_copy(spot, spot, sem).wait()

    class Ring:
        def __init__(self, view, me, ring, start, count):
            self.view, self.me, self.ring, self.start_row, self.count = view, me, ring, start, count

        def unit(self, step, half=None):
            lo, n = (0, self.count) if half is None else (half * self.count // 2, self.count // 2)
            return self.view(wrap(self.me + step, SIDE), pl.ds(self.start_row + lo, n))

        def own(self, group, stage):
            unit = self.unit(0)
            launch(group, stage, unit, unit, self.ring(1))
            launch(group, stage, unit, unit, self.ring(SIDE - 1))

        def onward(self, group, stage):
            first, second = self.unit(SIDE - 1, 0), self.unit(1, 1)
            launch(group, stage, first, first, self.ring(1))
            launch(group, stage, second, second, self.ring(SIDE - 1))

    class Rows:
        def __init__(self, start, rows, group):
            self.group, self.count = group, rows // 2
            a, b = (start, self.count), (start + self.count, self.count)
            self.rings = (
                (
                    Ring(lambda i, at: x_all.at[my, i, at], mx, x_ring, *a),
                    Ring(lambda i, at: x_all.at[i, mx, at], my, y_ring, *b),
                ),
                (
                    Ring(lambda i, at: x_all.at[i, :, at], my, y_ring, *a),
                    Ring(lambda i, at: x_all.at[:, i, at], mx, x_ring, *b),
                ),
            )

        def arrive(self):
            pass

        def gather_start(self, phase):
            for ring in self.rings[phase]:
                ring.own(self.group, 2 * phase)

        def gather_relay(self, phase):
            await_rows(recv_of(self.group, 2 * phase), (4, 16)[phase], self.count)
            for ring in self.rings[phase]:
                ring.onward(self.group, 2 * phase + 1)

        def gather_finish(self, phase):
            await_rows(recv_of(self.group, 2 * phase + 1), (2, 8)[phase], self.count)

    narrow = pin.shape[0]

    def mix_local():
        loads["xm"].wait()
        row_norm(xm, mix_gain_ref, mm)
        loads["pin"].wait()
        pooled_in = lax.dot_general(mm[...], pin[...], (((1,), (1,)), ((), ())), preferred_element_type=F32)
        pooled_in = jnp.concatenate([pooled_in, jnp.zeros((tok, LANES - narrow), F32)], axis=1).astype(BF16)
        halo_out[...] = pooled_in[tok - 16:, :]
        halo = pltpu.make_async_remote_copy(
            src_ref=halo_out, dst_ref=halo_in, send_sem=sq_send.at[1], recv_sem=sq_recv.at[1],
            device_id={"ep": wrap(ep + 1, n_ep), "tp": tp}, device_id_type=MESH,
        )
        halo.start()
        return pooled_in, halo

    def windows(pooled_in, halo):
        halo.wait_recv()
        carried = jnp.where(ep > 0, halo_in[...].astype(F32), 0.0)
        ext = jnp.concatenate([carried, pooled_in.astype(F32)], axis=0)
        sums, chosen, window = ext, None, 1
        for index in range(4):
            sums = sums + pltpu.roll(sums, window, 0)
            window *= 2
            chosen = sums if chosen is None else jnp.where(my >= index, sums, chosen)
        position = (ep * tok + lax.broadcasted_iota(jnp.int32, (tok, LANES), 0) + 1).astype(F32)
        widest = lax.shift_left(2, my).astype(F32)
        zeros_right = jnp.zeros((1, LANES - narrow), F32)
        pscale = jnp.concatenate([pscale_ref[...], zeros_right], axis=1)
        pgain = jnp.concatenate([pgain_ref[...], zeros_right], axis=1)
        scaled = (chosen[16:, :] / jnp.minimum(position, widest) - pooled_in.astype(F32)) * pscale
        squares = jnp.sum(scaled * scaled, axis=1, keepdims=True)
        squares = jnp.broadcast_to(squares, (tok, LANES)).T[0:8, :]
        sq_out[...] = squares

        for i in range(1, n_tp):
            pltpu.make_async_remote_copy(
                src_ref=sq_out, dst_ref=sq_in.at[i - 1], send_sem=sq_send.at[0], recv_sem=sq_recv.at[0],
                device_id={"ep": ep, "tp": wrap(tp + i, n_tp)}, device_id_type=MESH,
            ).start()
        return scaled, squares, pgain

    def combine_terms():
        high = weight.astype(BF16).astype(F32)
        low = weight - high
        for i in range(n_ep):
            at = slice(i * cap, (i + 1) * cap)
            same = place[i:i + 1, :] == slot_row
            chi[at, :] = jnp.where(same, high[i:i + 1, :], 0.0).astype(BF16)
            clo[at, :] = jnp.where(same, low[i:i + 1, :], 0.0).astype(BF16)

    pool_start = rows_all + tok

    def pool_norm(scaled, squares, pgain):
        pltpu.make_async_copy(sq_in, sq_in, sq_recv.at[0]).wait()
        total = squares
        for i in range(n_tp - 1):
            total = total + sq_in[i]
        total = jnp.broadcast_to(total[0:1, :], (tok, LANES)).T
        pooled = (scaled * lax.rsqrt(total / (narrow * n_tp) + EPS) * pgain).astype(BF16).astype(F32)
        packed = pooled[:tok // 2, :] + pltpu.roll(pooled[tok // 2:, :], narrow, 1)
        x_all[my, mx, pool_start:pool_start + tok // 2, :] = packed.astype(BF16)

    count = rows_all // (2 * n_pairs)
    half = count // 2

    class RingSum:
        def __init__(self, view, me, ring, opp, main, start):
            self.view, self.me, self.ring, self.opp, self.main, self.start_row = view, me, ring, opp, main, start

        def unit(self, step, which=None):
            lo, n = (0, count) if which is None else (which * half, half)
            return self.view(wrap(self.me + step, SIDE), pl.ds(self.start_row + lo, n))

        def into(self, side, which):
            at = pl.ds(which * half, half)
            return self.main.at[(side,) + (slice(None),) * (len(self.main.shape) - 3) + (at,)]

        def across(self, group, stage):
            launch(group, stage, self.unit(2, 0), self.opp.at[0], self.ring(1))
            launch(group, stage, self.unit(2, 1), self.opp.at[1], self.ring(SIDE - 1))

        def plain(self, group, stage):
            launch(group, stage, self.unit(1, 1), self.into(0, 1), self.ring(1))
            launch(group, stage, self.unit(SIDE - 1, 0), self.into(1, 0), self.ring(SIDE - 1))

        def added(self, group, stage):
            for unit, extra, dst, where in (
                (self.unit(1, 0), self.opp.at[0], self.into(0, 0), self.ring(1)),
                (self.unit(SIDE - 1, 1), self.opp.at[1], self.into(1, 1), self.ring(SIDE - 1)),
            ):
                unit[...] = (unit[...].astype(F32) + extra[...].astype(F32)).astype(BF16)
                launch(group, stage, unit, dst, where)

        def total(self, dst):
            own = self.unit(0)
            dst[...] = (own[...].astype(F32) + self.main[0].astype(F32) + self.main[1].astype(F32)).astype(BF16)

    tile = min(256, 2 * count)

    def experts(start, rows):
        @pl.loop(0, rows // tile)
        def _(b):
            at = pl.ds(pl.multiple_of(start + b * tile, tile), tile)
            lhs = jnp.concatenate([x_all[i // SIDE, i % SIDE, at, :] for i in range(n_tp)], axis=1)
            pair = dot(lhs, wgu[...])
            hidden = silu_mul(pair[:, :LANES], pair[:, LANES:]).astype(BF16)
            for j in range(n_tp // 2):
                out = dot(hidden, wd[:, j * 2 * LANES:(j + 1) * 2 * LANES])
                for s in range(2):
                    i = 2 * j + s
                    part[i // SIDE, i % SIDE, at, :] = out[:, s * LANES:(s + 1) * LANES].astype(BF16)

    class Pair(Rows):
        def __init__(self, k):
            self.k, self.chunks = k, (low_order[k], high_order[k])
            self.chunk = by_half(*self.chunks)
            self.start = self.chunk * (2 * count)
            if k > 0:
                self.start = pl.multiple_of(self.start, 2 * count)
            super().__init__(self.start, 2 * count, k)
            self.sums = (
                (
                    RingSum(lambda i, at: part.at[i, :, at], my, y_ring, opp1.at[0, k], main1.at[0, k], self.start),
                    RingSum(
                        lambda i, at: part.at[:, i, at], mx, x_ring, opp1.at[1, k], main1.at[1, k], self.start + count
                    ),
                ),
                (
                    RingSum(lambda i, at: q_a.at[k, i, at], mx, x_ring, opp2.at[0, k], main2.at[0, k], 0),
                    RingSum(lambda i, at: q_b.at[k, i, at], my, y_ring, opp2.at[1, k], main2.at[1, k], 0),
                ),
            )

        def arrive(self):
            lo = cap if self.k == 0 else 0
            got = x_all.at[my, mx, pl.ds(self.start + lo, 2 * count - lo)]
            pltpu.make_async_copy(got, got, z_recv.at[self.chunk]).wait()

        def compute(self):
            if self is pairs[0]:
                for name in ("eg", "eu", "ed"):
                    loads[name].wait()
            experts(self.start, 2 * count)

        def sum_start(self, phase):
            for ring in self.sums[phase]:
                ring.across(self.group, 4 + 2 * phase)
            for ring in self.sums[phase]:
                ring.plain(self.group, 5 + 2 * phase)

        def sum_relay(self, phase):
            await_rows(recv_of(self.group, 4 + 2 * phase), (8, 2)[phase], count)
            for ring in self.sums[phase]:
                ring.added(self.group, 5 + 2 * phase)

        def sum_finish(self, phase):
            await_rows(recv_of(self.group, 5 + 2 * phase), (16, 4)[phase], count)
            if phase == 0:
                targets = q_a.at[self.k], q_b.at[self.k]
            else:
                targets = y_own.at[pl.ds(self.start, count)], y_own.at[pl.ds(self.start + count, count)]
            for ring, dst in zip(self.sums[phase], targets):
                ring.total(dst)

        def send_back(self):
            if self.k == 0:
                back[0:cap, :] = y_own[0:cap, :]
            for i in range(self.k == 0, per_pair):
                at = pl.ds(pl.multiple_of(self.start + i * cap, cap), cap)
                low, high = (peer(chunk * per_pair + i) for chunk in self.chunks)
                pltpu.make_async_remote_copy(
                    src_ref=y_own.at[at], dst_ref=back.at[at], send_sem=zb_send, recv_sem=zb_recv,
                    device_id={"ep": by_half(low, high), "tp": tp}, device_id_type=MESH,
                ).start()

    pairs = [Pair(k) for k in range(n_pairs)]

    def plain_outputs():
        items[0].gather_finish(1)
        items[-1].gather_finish(1)
        for name in ("po_a", "po_b", "sd"):
            loads[name].wait()
        lane = lax.broadcasted_iota(jnp.int32, (tok // 2, LANES), 1)
        zero = jnp.zeros((tok // 2, LANES), BF16)
        upper, lower = [], []
        for i in range(n_tp):
            block = x_all[i // SIDE, i % SIDE, pool_start:pool_start + tok // 2, :]
            upper.append(jnp.where(lane < narrow, block, zero))
            lower.append(jnp.where(lane < narrow, zero, block))
        lhs = jnp.concatenate([jnp.concatenate(upper, axis=1), jnp.concatenate(lower, axis=1)], axis=0)
        out_ref[0] = dot(lhs, po2[...].reshape(2 * n_tp * narrow, LANES)).astype(BF16)
        lhs = jnp.concatenate([x_all[i // SIDE, i % SIDE, shared_rows, :] for i in range(n_tp)], axis=1)
        result = dot(lhs, sd[...])
        return result

    items = [Rows(rows_all, tok, n_pairs)] + pairs + [Rows(pool_start, tok // 2, n_pairs + 1)]

    def gathered(index):
        return items[index] if 0 <= index < len(items) else None

    def summed(index):
        return pairs[index - 1] if 1 <= index <= n_pairs else None

    for s in range(n_pairs + 1 + LAGS["close"]):
        if s == POOL_TICK:
            pool_norm(*pool_state)
        if p := gathered(s - LAGS["along"]):
            p.gather_finish(0)
            p.gather_start(1)
        if p := gathered(s - LAGS["relay"]):
            p.gather_relay(0)
        if p := gathered(s - LAGS["along_relay"]):
            p.gather_relay(1)
        if p := gathered(s):
            p.arrive()
            p.gather_start(0)
        if s in DISPATCH_TICKS:
            dispatch_later(DISPATCH_TICKS.index(s))
        if s == 0:
            pooled_in, halo = mix_local()
        if s == 2:
            combine_terms()
        if s == WINDOW_TICK:
            pool_state = windows(pooled_in, halo)
        if p := summed(s - LAGS["close"]):
            p.sum_finish(1)
            p.send_back()
        if s == n_pairs - 1 + LAGS["second_relay"]:
            result = plain_outputs()
        if p := summed(s - LAGS["second_relay"]):
            p.sum_relay(1)
        if p := summed(s - LAGS["second"]):
            p.sum_finish(0)
            p.sum_start(1)
        if p := summed(s - LAGS["first_relay"]):
            p.sum_relay(0)
        if p := summed(s - LAGS["compute"]):
            p.gather_finish(1)
            p.compute()
            p.sum_start(0)

    over = (((0,), (0,)), ((), ()))
    arrived = back.at[pl.ds(cap, rows_all - cap)]
    pltpu.make_async_copy(arrived, arrived, zb_recv).wait()
    result += lax.dot_general(chi[...], back[...], over, preferred_element_type=F32)
    result += lax.dot_general(clo[...], back[...], over, preferred_element_type=F32)
    out_ref[1] = result.astype(BF16)

    halo.wait_send()
    sent = [part.at[0:2, :, 0:30 * count]] * 4 + [part.at[0, 0:2, 0:15 * p.count] for p in (items[0], items[-1])]
    for at, gone in enumerate(sent):
        pltpu.make_async_copy(gone, gone, send_sems.at[at]).wait()
    for whole, sem in ((outgoing, z_send), (y_own, zb_send)):
        gone = whole.at[pl.ds(cap, rows_all - cap)]
        pltpu.make_async_copy(gone, gone, sem).wait()
    pltpu.make_async_copy(sq_in, sq_in, sq_send.at[0]).wait()


def on_device(n_pairs, mix_input, expert_input, mix_gain, moe_gain, pool_in, pool_scale, pool_gain, pool_out, route,
              route_score, expert_gate, expert_up, expert_down, shared_gate, shared_up, shared_down):
    n_ep, n_tp = lax.axis_size("ep"), lax.axis_size("tp")
    tok, width = mix_input.shape
    top = route.shape[1]
    cap = 2 * tok * top // n_ep
    rows = cap * n_ep
    narrow = pool_in.shape[1]
    count = rows // (2 * n_pairs)
    everything = rows + tok + tok // 2
    vmem = pl.BlockSpec(memory_space=pltpu.VMEM)
    hbm = pl.BlockSpec(memory_space=pltpu.HBM)
    dma = pltpu.SemaphoreType.DMA
    both = pl.pallas_call(
        functools.partial(kernel, n_pairs),
        out_shape=jax.ShapeDtypeStruct((2, tok, shared_down.shape[1]), BF16),
        in_specs=[hbm, hbm, vmem, vmem, hbm, vmem, vmem, hbm, vmem, vmem, hbm, hbm, hbm, hbm, hbm, hbm],
        out_specs=vmem,
        scratch_shapes=[
            pltpu.VMEM((tok, width), BF16),
            pltpu.VMEM((tok, width), BF16),
            pltpu.VMEM((width, 2 * LANES), BF16),
            pltpu.VMEM((LANES, width), BF16),
            pltpu.VMEM((width, 2 * LANES), BF16),
            pltpu.VMEM((width, LANES), BF16),
            pltpu.VMEM((narrow, width), BF16),
            pltpu.VMEM((n_tp, 2, narrow, LANES), BF16),
            pltpu.VMEM((tok, width), BF16),
            pltpu.VMEM((tok, width), BF16),
            pltpu.VMEM((rows, LANES), BF16),
            pltpu.VMEM((rows, LANES), BF16),
            pltpu.VMEM((rows, LANES), BF16),
            pltpu.VMEM((rows, LANES), BF16),
            pltpu.VMEM((SIDE, SIDE, everything, LANES), BF16),
            pltpu.VMEM((SIDE, SIDE, rows, LANES), BF16),
            pltpu.VMEM((n_pairs, SIDE, count, LANES), BF16),
            pltpu.VMEM((n_pairs, SIDE, count, LANES), BF16),
            pltpu.VMEM((rows, LANES), BF16),
            pltpu.VMEM((rows, LANES), BF16),
            pltpu.VMEM((2, n_pairs, 2, SIDE, count // 2, LANES), BF16),
            pltpu.VMEM((2, n_pairs, 2, SIDE, count, LANES), BF16),
            pltpu.VMEM((2, n_pairs, 2, count // 2, LANES), BF16),
            pltpu.VMEM((2, n_pairs, 2, count, LANES), BF16),
            pltpu.VMEM((16, LANES), BF16),
            pltpu.VMEM((16, LANES), BF16),
            pltpu.VMEM((8, LANES), F32),
            pltpu.VMEM((n_tp - 1, 8, LANES), F32),
            dma((11,)),
            dma((6,)),
            dma((n_pairs // 2, 8)),
            dma((2, 4)),
            dma,
            dma((n_pairs,)),
            dma,
            dma,
            dma((2,)),
            dma((2,)),
        ],
        compiler_params=pltpu.CompilerParams(
            collective_id=0, has_side_effects=True, vmem_limit_bytes=60 * 1024 * 1024
        ),
    )(
        expert_input,
        mix_input,
        mix_gain.reshape(1, -1),
        moe_gain.reshape(1, -1),
        pool_in.T,
        pool_scale.reshape(1, -1),
        pool_gain.reshape(1, -1),
        pool_out.reshape(n_tp, narrow, pool_out.shape[1]),
        route.T,
        route_score.T,
        expert_gate,
        expert_up,
        expert_down,
        shared_gate,
        shared_up,
        shared_down,
    )
    return both[0], both[1]


def solution(mesh):
    return jax.shard_map(
        functools.partial(on_device, 16),
        mesh=mesh,
        in_specs=(
            P("ep", None),
            P("ep", None),
            P(),
            P(),
            P(None, "tp"),
            P("tp"),
            P("tp"),
            P(None, "tp"),
            P("ep", None),
            P("ep", None),
            P("ep", None, "tp"),
            P("ep", None, "tp"),
            P("ep", "tp", None),
            P(None, "tp"),
            P(None, "tp"),
            P(None, "tp"),
        ),
        out_specs=(P("ep", "tp"), P("ep", "tp")),
        check_vma=False,
    )
```
